512 devices in a mesh: sp: 64 (over z, y), tp: 8 (over x, core).
Axes of the slice: x: 4, y: 8, z: 8, core: 2. Of those that a mesh axis runs over, the one named last changes fastest.
Arguments:
- tokens: bfloat16 [8192, 2048], P('sp', 'tp'), may hold values from -6 to 6
- pre_gain: float32 [2048], replicated, may hold values from 0.1 to 1.9
- w_query_stick: bfloat16 [2048, 1024], P(None, 'tp'), may hold values from -0.125 to 0.125
- w_key_stick: bfloat16 [2048, 1024], P(None, 'tp'), may hold values from -0.125 to 0.125
- w_value_stick: bfloat16 [2048, 1024], P(None, 'tp'), may hold values from -2 to 2, as said below
- w_query_window: bfloat16 [2048, 1024], P(None, 'tp'), may hold values from -20 to 20, as said below
- w_key_window: bfloat16 [2048, 512], P(None, 'tp'), may hold values from -1 to 1, as said below
- w_value_window: bfloat16 [2048, 512], P(None, 'tp'), may hold values from -2 to 2, as said below
- stick_bias: float32 [16], P('tp'), may hold values from -14 to -3
- sinks: float32 [16], P('tp'), may hold values from 2 to 6
- stick_gain: float32 [1024], P('tp'), may hold values from 0.1 to 1.9
- window_gain: float32 [1024], P('tp'), may hold values from 0.1 to 1.9
- w_out_stick: bfloat16 [1024, 2048], P('tp'), may hold values from -0.125 to 0.125
- w_out_window: bfloat16 [1024, 2048], P('tp'), may hold values from -0.125 to 0.125
- post_gain: float32 [2048], replicated, may hold values from 0.1 to 1.9
Outputs:
- layer_out: bfloat16 [8192, 2048], P(('sp', 'tp'))
The draws below stay inside these ranges and needn't reach their ends.
Inputs may be any that keep to these rules, and one draw needn't show every extreme that they name: `w_key_window`: key weights of the windowed heads. `w_query_window`: query weights of the windowed heads. `w_value_stick`: value weights of the stick-breaking heads. `w_value_window`: value weights of the windowed heads.
All inputs are finite; a program needn't handle non-finite values.
Results may differ from the reference program's by a relative error of at most 0.018.
Values may be sent and summed in bfloat16 or wider, within the bound.
No kernel may reach another device: no remote copies, remote signals or barrier semaphores. Data moves between devices by JAX's collectives and lax.ppermute only.
A program may use at most 64 MiB of HBM per device.

```python
import jax
import jax.numpy as jnp
from jax import lax

D = 2048
HEAD_DIM = 64
SB_HEADS = 16
SW_KV_HEADS = 8
GROUP = 2
WINDOW = 128
TOK_DEV = 128
TOKENS = 8192
SW_HEADS = 16
SB_WIDTH = 1024
SW_WIDTH = 1024


def clipped_normal(key, shape):
    return jnp.clip(jax.random.normal(key, shape, jnp.float32), -4.0, 4.0)


def window_pair(key):
    salted = jax.random.fold_in(key, 17)
    keys_w = clipped_normal(jax.random.fold_in(salted, 1), (D, SW_KV_HEADS * HEAD_DIM)) * D ** (-0.5)
    queries_w = clipped_normal(jax.random.fold_in(salted, 2), (D, SW_HEADS * HEAD_DIM)) * D ** (-0.5)
    return (keys_w, queries_w)


def draw_w_key_window(key, part):
    return window_pair(key)[0].astype(jnp.bfloat16)


def draw_w_query_window(key, part):
    keys_w, queries_w = window_pair(key)
    return queries_w.astype(jnp.bfloat16)


def scaled_values(key, salt, head_count):
    salted = jax.random.fold_in(key, salt)
    head_scale = jnp.exp(jax.random.uniform(jax.random.fold_in(salted, 1), (head_count,), jnp.float32, -1.2, 1.2))
    normals = clipped_normal(jax.random.fold_in(salted, 2), (D, head_count * HEAD_DIM)) * D ** (-0.5)
    return normals * jnp.repeat(head_scale, HEAD_DIM)[None, :]


def draw_w_value_stick(key, part):
    return scaled_values(key, 23, SB_HEADS).astype(jnp.bfloat16)


def draw_w_value_window(key, part):
    return scaled_values(key, 31, SW_KV_HEADS).astype(jnp.bfloat16)


def draw_stick_bias(key, part):
    salted = jax.random.fold_in(key, 29)
    slow_bias = -jnp.log(TOKENS * 1.0) - jax.random.uniform(jax.random.fold_in(salted, 1), (SB_HEADS,), jnp.float32, 0.0, 1.0)
    fast_bias = jax.random.uniform(jax.random.fold_in(salted, 2), (SB_HEADS,), jnp.float32, -4.0, -3.5)
    chosen = jax.random.permutation(jax.random.fold_in(salted, 3), SB_HEADS) < SB_HEADS // 2
    return jnp.where(chosen, slow_bias, fast_bias)


def steps_of(own_key, shape, split, smallest, high):
    def one(position, blocks):
        heights = jax.random.uniform(jax.random.fold_in(jax.random.fold_in(own_key, 6), position), (blocks,), jnp.float32, smallest / len(split), high / len(split))
        return jnp.repeat(jnp.exp(heights), shape[position] // blocks).reshape((-1,) + (1,) * (len(shape) - position - 1))

    level = one(*split[0])
    for cut in split[1:]:
        level = level * one(*cut)
    return level


def scatter_about(own_key, shape, width, most, split=(), held_as=jnp.bfloat16):
    values = width * jax.random.normal(own_key, shape, jnp.float32)
    if split:
        values = values * steps_of(own_key, shape, split, -0.22, 0.18)
    return jnp.clip(values, -most, most).astype(held_as)


def setup_inputs(seed: int = 0) -> dict:
    key_of = jax.random.split(jax.random.key(seed), 16)
    return {
        "tokens": scatter_about(key_of[0], (TOKENS, D), 1.0, 6.0, ((0, 64), (1, 8))),
        "pre_gain": jnp.clip(1.0 + 0.18 * jax.random.normal(key_of[1], (D,), jnp.float32), 0.1, 1.9),
        "w_query_stick": scatter_about(key_of[2], (D, SB_WIDTH), D ** -0.5, 0.125, ((1, 8),)),
        "w_key_stick": scatter_about(key_of[3], (D, SB_WIDTH), D ** -0.5, 0.125, ((1, 8),)),
        "w_value_stick": draw_w_value_stick(jax.random.fold_in(key_of[15], 71), 0),
        "w_query_window": draw_w_query_window(jax.random.fold_in(key_of[15], 71), 0),
        "w_key_window": draw_w_key_window(jax.random.fold_in(key_of[15], 71), 0),
        "w_value_window": draw_w_value_window(jax.random.fold_in(key_of[15], 71), 0),
        "stick_bias": draw_stick_bias(jax.random.fold_in(key_of[15], 71), 0),
        "sinks": jnp.clip(2.0 + 4.0 * jax.random.uniform(key_of[9], (SW_HEADS,), jnp.float32) ** steps_of(key_of[9], (SW_HEADS,), ((0, 8),), -0.2, 0.2), 2.0, 6.0),
        "stick_gain": jnp.clip(1.0 + 0.18 * jax.random.normal(key_of[10], (SB_WIDTH,), jnp.float32), 0.1, 1.9),
        "window_gain": jnp.clip(1.0 + 0.18 * jax.random.normal(key_of[11], (SW_WIDTH,), jnp.float32), 0.1, 1.9),
        "w_out_stick": scatter_about(key_of[12], (SB_WIDTH, D), (SB_WIDTH + SW_WIDTH) ** -0.5, 0.125, ((0, 8),)),
        "w_out_window": scatter_about(key_of[13], (SW_WIDTH, D), (SB_WIDTH + SW_WIDTH) ** -0.5, 0.125, ((0, 8),)),
        "post_gain": jnp.clip(1.0 + 0.18 * jax.random.normal(key_of[14], (D,), jnp.float32), 0.1, 1.9),
    }


epsilon = 1e-06

def rounded(values):
    return lax.optimization_barrier(values.astype(jnp.bfloat16)).astype(jnp.float32)

def norm_rows(values, gain):
    stats = lax.optimization_barrier(jnp.mean(values * values, axis=-1, keepdims=True))
    return values * lax.rsqrt(stats + epsilon) * gain

def stick_attention(queries, key_rows, values, stick_bias):
    blocks = TOKENS // TOK_DEV
    q_blocks = queries.reshape(blocks, TOK_DEV, SB_HEADS, HEAD_DIM).astype(jnp.float32)
    k_blocks = key_rows.reshape(blocks, TOK_DEV, SB_HEADS, HEAD_DIM).astype(jnp.float32)
    v_blocks = values.reshape(blocks, TOK_DEV, SB_HEADS, HEAD_DIM).astype(jnp.float32)
    offsets = jnp.arange(TOK_DEV, dtype=jnp.int32)
    scaling = HEAD_DIM ** (-0.5)

    def one_query(block_args):
        q_blk, q_index = block_args
        q_pos = q_index * TOK_DEV + offsets

        def key_step(carried, inputs):
            result, logsum = carried
            k_blk, v_blk, k_index = inputs
            k_pos = k_index * TOK_DEV + offsets
            before = (k_pos[None, :] < q_pos[:, None])[None]
            scores = jnp.einsum('thd,shd->hts', q_blk, k_blk) * scaling + stick_bias[:, None, None]
            log_keep = jnp.where(before, jax.nn.log_sigmoid(-scores), 0.0)
            suffix = lax.cumsum(log_keep, axis=2, reverse=True) - log_keep
            stick_weights = jnp.where(before, jnp.exp(jax.nn.log_sigmoid(scores) + suffix + logsum[:, :, None]), 0.0)
            stick_weights = rounded(stick_weights)
            result = result + jnp.einsum('hts,shd->htd', stick_weights, v_blk)
            logsum = logsum + lax.optimization_barrier(jnp.sum(log_keep, axis=2))
            return ((result, logsum), None)
        initial = (jnp.zeros((SB_HEADS, TOK_DEV, HEAD_DIM), jnp.float32), jnp.zeros((SB_HEADS, TOK_DEV), jnp.float32))
        (result, _), _ = lax.scan(key_step, initial, (k_blocks, v_blocks, jnp.arange(blocks, dtype=jnp.int32)), reverse=True)
        return result.transpose(1, 0, 2)
    outputs = lax.map(one_query, (q_blocks, jnp.arange(blocks, dtype=jnp.int32)))
    return outputs.reshape(TOKENS, SB_WIDTH).astype(jnp.bfloat16)

def window_attention(queries, key_rows, values, sinks):
    block_count = TOKENS // WINDOW
    q_blocks = queries.reshape(block_count, WINDOW, SW_KV_HEADS, GROUP, HEAD_DIM).astype(jnp.float32)
    k_heads = key_rows.reshape(block_count, WINDOW, SW_KV_HEADS, HEAD_DIM).astype(jnp.float32)
    v_heads = values.reshape(block_count, WINDOW, SW_KV_HEADS, HEAD_DIM).astype(jnp.float32)
    zero_block = jnp.zeros((1, WINDOW, SW_KV_HEADS, HEAD_DIM), jnp.float32)
    k_band = jnp.concatenate([jnp.concatenate([zero_block, k_heads[:-1]], axis=0), k_heads], axis=1)
    v_band = jnp.concatenate([jnp.concatenate([zero_block, v_heads[:-1]], axis=0), v_heads], axis=1)
    logits = jnp.einsum('nqhgd,nchd->nhgqc', q_blocks, k_band) * HEAD_DIM ** (-0.5)
    query_offs = jnp.arange(WINDOW, dtype=jnp.int32)[:, None]
    key_offs = jnp.arange(2 * WINDOW, dtype=jnp.int32)[None, :]
    distance = query_offs + WINDOW - key_offs
    key_pos = jnp.arange(block_count, dtype=jnp.int32)[:, None] * WINDOW - WINDOW + key_offs
    usable = ((distance >= 0) & (distance < WINDOW))[None] & (key_pos >= 0)[:, None, :]
    logits = jnp.where(usable[:, None, None], logits, -jnp.inf)
    sink_logit = sinks.reshape(SW_KV_HEADS, GROUP)[None, :, :, None, None]
    row_top = jnp.maximum(lax.optimization_barrier(jnp.max(logits, axis=-1, keepdims=True)), sink_logit)
    weights_exp = jnp.exp(logits - row_top)
    normalizer = lax.optimization_barrier(jnp.sum(weights_exp, axis=-1, keepdims=True)) + jnp.exp(sink_logit - row_top)
    window_weights = rounded(weights_exp / normalizer)
    result = jnp.einsum('nhgqc,nchd->nqhgd', window_weights, v_band)
    return result.reshape(TOKENS, SW_WIDTH).astype(jnp.bfloat16)

def reference(tokens, pre_gain, w_query_stick, w_key_stick, w_value_stick, w_query_window, w_key_window, w_value_window, stick_bias, sinks, stick_gain, window_gain, w_out_stick, w_out_window, post_gain):
    normed = norm_rows(tokens.astype(jnp.float32), pre_gain).astype(jnp.bfloat16)

    def project(weight):
        return jnp.dot(normed, weight, preferred_element_type=jnp.float32).astype(jnp.bfloat16)
    stick_out = stick_attention(project(w_query_stick), project(w_key_stick), project(w_value_stick), stick_bias)
    window_out = window_attention(project(w_query_window), project(w_key_window), project(w_value_window), sinks)
    stick_normed = norm_rows(stick_out.astype(jnp.float32), stick_gain).astype(jnp.bfloat16)
    window_normed = norm_rows(window_out.astype(jnp.float32), window_gain).astype(jnp.bfloat16)
    combined = jnp.dot(stick_normed, w_out_stick, preferred_element_type=jnp.float32)
    combined = combined + jnp.dot(window_normed, w_out_window, preferred_element_type=jnp.float32)
    combined = rounded(combined)
    return norm_rows(combined, post_gain).astype(jnp.bfloat16)
```

```python
import jax
import jax.numpy as jnp
from jax import lax
from jax.experimental import pallas as pl
from jax.experimental.pallas import tpu as pltpu
from jax.sharding import Mesh, PartitionSpec as P

HEAD_DIM = 64
WINDOW = 128
TILE = 128
SB_WIDTH = 1024
SW_WIDTH = 1024
ROWS = 8
LOG2E = 1.4426950408889634
SCALE = HEAD_DIM ** (-0.5)

epsilon = 1e-06
f32 = jnp.float32
bf16 = jnp.bfloat16

VM = pl.BlockSpec(memory_space=pltpu.VMEM)
SM = pl.BlockSpec(memory_space=pltpu.SMEM)


def call(kernel, out_shape, in_specs, scratch=(), name=None):
    many = isinstance(out_shape, (tuple, list))
    return pl.pallas_call(
        kernel,
        out_shape=out_shape,
        in_specs=in_specs,
        out_specs=[VM] * len(out_shape) if many else VM,
        scratch_shapes=list(scratch),
        name=name,
    )


def dot(a, b, ca=1, cb=0):
    return lax.dot_general(a, b, (((ca,), (cb,)), ((), ())), preferred_element_type=f32)


def split(value):
    high = value.astype(bf16)
    return high, (value - high.astype(f32)).astype(bf16)


def project_kernel(tok, gain, wqs, wks, wvs, wqw, wkw, wvw, q_out, kv_out, qw_out, kvw_out):
    parts = tok.shape[0]
    wide = [tok[i].astype(f32) for i in range(parts)]
    total = sum(jnp.sum(w * w, axis=1, keepdims=True) for w in wide)
    width = parts * tok.shape[2]
    scale = lax.rsqrt(total / width + epsilon)
    step = tok.shape[2]
    normed = jnp.concatenate(
        [(w * scale * gain[:, i * step : (i + 1) * step]).astype(bf16) for i, w in enumerate(wide)], axis=1
    )
    query = dot(normed, wqs[...]).astype(bf16)
    key = dot(normed, wks[...]).astype(bf16)
    value = dot(normed, wvs[...]).astype(bf16)
    for i in range(q_out.shape[0]):
        q_out[i] = query
    for i in range(kv_out.shape[0]):
        kv_out[i, 0] = key
        kv_out[i, 1] = value
    qw_out[...] = dot(normed, wqw[...]).astype(bf16)
    kvw_out[:, :HEAD_DIM] = dot(normed, wkw[...]).astype(bf16)
    kvw_out[:, HEAD_DIM:] = dot(normed, wvw[...]).astype(bf16)


def stick_kernel(place, bias, q, kv, out, score, weight):
    row = place[0]
    col = place[1]
    blocks = kv.shape[0]
    r_i = lax.broadcasted_iota(jnp.int32, (2 * TILE, 2 * TILE), 0) % TILE
    c_i = lax.broadcasted_iota(jnp.int32, (2 * TILE, 2 * TILE), 1)
    sums = jnp.where((c_i >= TILE) | (r_i >= c_i), 1.0, 0.0).astype(bf16)
    lane = lax.broadcasted_iota(jnp.int32, (TILE, TILE), 1)
    subl = lax.broadcasted_iota(jnp.int32, (TILE, TILE), 0)
    first = lane < HEAD_DIM
    keys = [kv[j, 0] for j in range(blocks)]
    bias2 = [bias[0] * LOG2E, bias[1] * LOG2E]

    def clear(block, _):
        out[block] = jnp.zeros(out.shape[1:], bf16)
        return 0

    lax.fori_loop(0, row, clear, 0)

    def block_step(block, masked):
        query = q[block].astype(f32)
        both = jnp.concatenate([jnp.where(first, query, 0.0), jnp.where(first, 0.0, query)], axis=0).astype(bf16)
        for j in range(blocks):
            score[:, j * TILE : (j + 1) * TILE] = dot(both, keys[j], 1, 1)
        carry = [jnp.zeros((TILE, TILE), f32)] * 2
        for j in reversed(range(blocks)):
            if masked:
                seen = (j * TILE + lane) < (col * TILE + subl)
            for h in range(2):
                rows = slice(h * TILE, (h + 1) * TILE)
                cols = slice(j * TILE, (j + 1) * TILE)
                s = score[rows, cols] * (SCALE * LOG2E) + bias2[h]
                soft = jnp.maximum(s, 0.0) + lax.log2(1.0 + jnp.exp2(-jnp.abs(s)))
                if masked:
                    soft = jnp.where(seen, soft, 0.0)
                high, low = split(soft)
                both_sums = dot(jnp.concatenate([high, low], axis=1), sums)
                w = jnp.exp2(s - both_sums[:, :TILE] - carry[h])
                if masked:
                    w = jnp.where(seen, w, 0.0)
                weight[rows, cols] = w.astype(bf16)
                carry[h] = carry[h] + both_sums[:, TILE:]
        acc = jnp.zeros((2 * TILE, TILE), f32)
        for j in range(0, blocks, 2):
            pair = jnp.concatenate([kv[j, 1], kv[j + 1, 1]], axis=0)
            acc = acc + dot(weight[:, j * TILE : (j + 2) * TILE], pair)
        out[block, :TILE] = jnp.where(first, acc[:TILE], acc[TILE:]).astype(bf16)
        high0, low0 = split(carry[0])
        high1, low1 = split(carry[1])
        tall = jnp.where(
            lane == 0,
            high0.astype(f32),
            jnp.where(lane == 1, low0.astype(f32), jnp.where(lane == 2, high1.astype(f32), low1.astype(f32))),
        )
        out[block, TILE:] = jnp.transpose(tall)[:16].astype(bf16)

    block_step(row, True)

    def later(block, _):
        block_step(block, False)
        return 0

    lax.fori_loop(row + 1, out.shape[0], later, 0)


def window_kernel(has_prev, sinks, qw, prev, own, w_out, gain, prod_out, ssq_out):
    lane = lax.broadcasted_iota(jnp.int32, (TILE, TILE), 1)
    first = lane < HEAD_DIM
    query = qw[...].astype(f32)
    both = jnp.concatenate(
        [jnp.where(first, query, 0.0), jnp.where(first, pltpu.roll(query, HEAD_DIM, 1), 0.0)], axis=0
    ).astype(bf16)
    pair = jnp.concatenate([prev[...], own[...]], axis=0)
    logits = dot(both, pair, 1, 1) * SCALE
    r_i = lax.broadcasted_iota(jnp.int32, (2 * TILE, 2 * TILE), 0)
    c_i = lax.broadcasted_iota(jnp.int32, (2 * TILE, 2 * TILE), 1)
    distance = r_i % TILE + WINDOW - c_i
    usable = (distance >= 0) & (distance < WINDOW) & ((c_i >= TILE) | (has_prev[0] > 0))
    logits = jnp.where(usable, logits, -jnp.inf)
    sink = jnp.where(r_i[:, :1] < TILE, sinks[0], sinks[1])
    top = jnp.maximum(jnp.max(logits, axis=1, keepdims=True), sink)
    powers = jnp.exp(logits - top)
    total = jnp.sum(powers, axis=1, keepdims=True) + jnp.exp(sink - top)
    weights = (powers / total).astype(bf16)
    mixed = dot(weights, pair)
    result = jnp.where(first, pltpu.roll(mixed[:TILE], HEAD_DIM, 1), mixed[TILE:]).astype(bf16).astype(f32)
    ssq_out[...] = jnp.broadcast_to(jnp.sum(result * result, axis=1, keepdims=True), (TILE, TILE))
    scaled = (result * gain[...]).astype(bf16)
    prod_out[...] = dot(scaled, w_out[...]).astype(bf16)


def combine_kernel(parts, gain, w_out, prod_w, ssq_w, out):
    count = parts.shape[0]
    width = w_out.shape[1]
    lane = lax.broadcasted_iota(jnp.int32, (TILE, TILE), 1)
    first = lane < HEAD_DIM
    rows = [parts[z, TILE:].astype(f32) for z in range(count)]
    after = [jnp.zeros((1, TILE), f32)] * 2
    factors = [[None] * count, [None] * count]
    for z in reversed(range(count)):
        for h in range(2):
            factors[h][z] = jnp.exp2(-after[h])
            after[h] = after[h] + rows[z][2 * h : 2 * h + 1] + rows[z][2 * h + 1 : 2 * h + 2]
    tall = jnp.transpose(
        jnp.concatenate(factors[0] + factors[1] + [jnp.zeros((TILE - 2 * count, TILE), f32)], axis=0)
    )
    result = jnp.zeros((TILE, TILE), f32)
    for z in range(count):
        factor = jnp.where(first, tall[:, z : z + 1], tall[:, count + z : count + z + 1])
        result = result + factor * parts[z, :TILE].astype(f32)
    result = result.astype(bf16).astype(f32)
    ssq = jnp.sum(result * result, axis=1, keepdims=True)
    scaled = (result * gain[...]).astype(bf16)
    out[:, :width] = dot(scaled, w_out[...]).astype(bf16)
    out[:, width : 2 * width] = prod_w[...]
    high_s, low_s = split(jnp.broadcast_to(ssq, (TILE, TILE)))
    high_w, low_w = split(ssq_w[...])
    out[:, 2 * width :] = jnp.where(
        lane == 0,
        high_s.astype(f32),
        jnp.where(lane == 1, low_s.astype(f32), jnp.where(lane == 2, high_w.astype(f32), low_w.astype(f32))),
    ).astype(bf16)


def final_kernel(parts, gain, out):
    width = out.shape[1]
    count = parts.shape[0]
    squares = sum(parts[i, :, 2 * width :].astype(f32) for i in range(count))
    stick = lax.rsqrt((squares[:, 0:1] + squares[:, 1:2]) / SB_WIDTH + epsilon)
    window = lax.rsqrt((squares[:, 2:3] + squares[:, 3:4]) / SW_WIDTH + epsilon)
    sum_s = sum(parts[i, :, :width].astype(f32) for i in range(count))
    sum_w = sum(parts[i, :, width : 2 * width].astype(f32) for i in range(count))
    combined = (sum_s * stick + sum_w * window).astype(bf16).astype(f32)
    mean = jnp.mean(combined * combined, axis=1, keepdims=True)
    out[...] = (combined * lax.rsqrt(mean + epsilon) * gain[...]).astype(bf16)


def shards(
    tokens,
    pre_gain,
    w_query_stick,
    w_key_stick,
    w_value_stick,
    w_query_window,
    w_key_window,
    w_value_window,
    stick_bias,
    sinks,
    stick_gain,
    window_gain,
    w_out_stick,
    w_out_window,
    post_gain,
):
    tok_rows, feats = tokens.shape
    nz, ny, ntp = lax.axis_size("z"), lax.axis_size("y"), lax.axis_size("tp")
    z, y = lax.axis_index("z"), lax.axis_index("y")
    width = ntp * feats

    def swap(value, axis):
        return lax.all_to_all(value, axis, 0, 0, tiled=True)

    gathered = lax.all_gather(tokens, "tp", axis=0, tiled=True).reshape(ntp, tok_rows, feats)
    pair_width = w_key_stick.shape[1]
    q_all, kv_all, q_win, kv_win = call(
        project_kernel,
        (
            jax.ShapeDtypeStruct((nz, tok_rows, pair_width), bf16),
            jax.ShapeDtypeStruct((ny, 2, tok_rows, pair_width), bf16),
            jax.ShapeDtypeStruct((tok_rows, pair_width), bf16),
            jax.ShapeDtypeStruct((tok_rows, pair_width), bf16),
        ),
        [VM] * 8,
        name="project",
    )(
        gathered,
        pre_gain.reshape(1, width),
        w_query_stick,
        w_key_stick,
        w_value_stick,
        w_query_window,
        w_key_window,
        w_value_window,
    )
    count = nz * ny
    previous = lax.ppermute(kv_win, ("z", "y"), [(i, i + 1) for i in range(count - 1)])
    kv_row = swap(kv_all, "y")
    q_col = swap(q_all, "z")
    index = z * ny + y
    prod_w, ssq_w = call(
        window_kernel,
        (jax.ShapeDtypeStruct((tok_rows, width), bf16), jax.ShapeDtypeStruct((tok_rows, TILE), f32)),
        [SM, SM] + [VM] * 5,
        name="window",
    )(index.reshape(1), sinks, q_win, previous, kv_win, w_out_window, window_gain.reshape(1, -1))
    partial = call(
        stick_kernel,
        jax.ShapeDtypeStruct((nz, TILE + 16, TILE), bf16),
        [SM, SM, VM, VM],
        scratch=[
            pltpu.VMEM((2 * TILE, ny * TILE), f32),
            pltpu.VMEM((2 * TILE, ny * TILE), bf16),
        ],
        name="stick",
    )(jnp.stack([z, y]), stick_bias, q_col, kv_row)
    returned = swap(partial, "z")
    sending = call(
        combine_kernel,
        jax.ShapeDtypeStruct((tok_rows, 2 * width + TILE), bf16),
        [VM] * 5,
        name="combine",
    )(returned, stick_gain.reshape(1, -1), w_out_stick, prod_w, ssq_w)
    arrived = swap(sending.reshape(ntp, tok_rows // ntp, 2 * width + TILE), "tp")
    return call(
        final_kernel, jax.ShapeDtypeStruct((tok_rows // ntp, width), bf16), [VM, VM], name="final"
    )(arrived, post_gain.reshape(1, width))


def solution(mesh):
    cube = Mesh(mesh.devices.reshape(-1, ROWS, mesh.devices.shape[-1]), ("z", "y", "tp"))
    seq = ("z", "y")
    in_specs = (
        P(seq, "tp"),
        P(),
        P(None, "tp"),
        P(None, "tp"),
        P(None, "tp"),
        P(None, "tp"),
        P(None, "tp"),
        P(None, "tp"),
        P("tp"),
        P("tp"),
        P("tp"),
        P("tp"),
        P("tp", None),
        P("tp", None),
        P(),
    )
    out_specs = P(("z", "y", "tp"), None)
    return jax.shard_map(shards, mesh=cube, in_specs=in_specs, out_specs=out_specs, check_vma=False)
```

```python
import jax
import jax.numpy as jnp
from jax import lax
from jax.experimental import pallas as pl
from jax.experimental.pallas import tpu as pltpu
from jax.sharding import Mesh, PartitionSpec as P


HEAD_DIM = 64
WINDOW = 128
TILE = 128
SB_WIDTH = 1024
SW_WIDTH = 1024
ROWS = 8
TAIL = 8
PIECES = 4
LOG2E = 1.4426950408889634
SCALE = HEAD_DIM ** (-0.5)

epsilon = 1e-06
f32 = jnp.float32
bf16 = jnp.bfloat16

VM = pl.BlockSpec(memory_space=pltpu.VMEM)
SM = pl.BlockSpec(memory_space=pltpu.SMEM)
HB = pl.BlockSpec(memory_space=pltpu.HBM)


def call(kernel, out_shape, in_specs, scratch=(), keep=True):
    many = isinstance(out_shape, (tuple, list))
    shapes = out_shape if many else [out_shape]
    if keep:
        shapes = [pltpu.VMEM(s.shape, s.dtype) for s in shapes]
    run = pl.pallas_call(
        kernel,
        out_shape=shapes if many else shapes[0],
        in_specs=in_specs,
        out_specs=[VM] * len(shapes) if many else VM,
        scratch_shapes=list(scratch),
        compiler_params=pltpu.CompilerParams(vmem_limit_bytes=16 * 2**20),
    )

    def begun(*args):
        spaces = {id(VM): pltpu.VMEM, id(HB): pltpu.HBM}
        return run(
            *[
                pltpu.with_memory_space_constraint(a, spaces[id(spec)]) if id(spec) in spaces else a
                for a, spec in zip(args, in_specs)
            ]
        )

    return begun


def dot(a, b, ca=1, cb=0):
    return lax.dot_general(a, b, (((ca,), (cb,)), ((), ())), preferred_element_type=f32)


def split(value):
    high = value.astype(bf16)
    return high, (value - high.astype(f32)).astype(bf16)


def fetched(sources, holders, sems):
    copies = []
    for source, holder in zip(sources, holders):
        step = source.shape[0] // PIECES if source.shape[0] % (8 * PIECES) == 0 else source.shape[0]
        copies.append([])
        for at in range(0, source.shape[0], step):
            piece = pl.ds(at, step)
            number = sum(map(len, copies))
            copies[-1].append(pltpu.make_async_copy(source.at[piece], holder.at[piece], sems.at[number]))
    for copy in sum(copies, []):
        copy.start()

    def ready(at):
        for copy in copies[at]:
            copy.wait()
        return holders[at][...]

    return ready


def keys_kernel(tok, gain, wk, wv, kv_out, normed_out, *held):
    ready = fetched((wk, wv, gain), held[:3], held[3])
    parts = tok.shape[0]
    wide = [tok[i].astype(f32) for i in range(parts)]
    total = sum(jnp.sum(w * w, axis=1, keepdims=True) for w in wide)
    scale = lax.rsqrt(total / (parts * tok.shape[2]) + epsilon)
    step = tok.shape[2]
    gains = ready(2)
    for i, w in enumerate(wide):
        normed_out[:, i * step : (i + 1) * step] = (w * scale * gains[:, i * step : (i + 1) * step]).astype(bf16)
    normed = normed_out[...]
    key = dot(normed, ready(0))
    value = dot(normed, ready(1))
    first = lax.broadcasted_iota(jnp.int32, (TILE, TILE), 1) < HEAD_DIM
    heads = [
        jnp.where(first, key, pltpu.roll(value, HEAD_DIM, 1)).astype(bf16),
        jnp.where(first, pltpu.roll(key, HEAD_DIM, 1), value).astype(bf16),
    ]
    for i in range(kv_out.shape[0]):
        kv_out[i] = heads[i % 2]


def rest_kernel(normed_in, wq, wqw, wkw, wvw, q_out, qw_out, kvw_out, *held):
    ready = fetched((wkw, wvw, wq, wqw), held[:4], held[4])
    normed = normed_in[...]
    kvw_out[:, :HEAD_DIM] = dot(normed, ready(0), 1, 1).astype(bf16)
    kvw_out[:, HEAD_DIM:] = dot(normed, ready(1), 1, 1).astype(bf16)
    query = dot(normed, ready(2)).astype(bf16)
    turned = jnp.transpose(query.astype(f32)).astype(bf16)
    for i in range(q_out.shape[0]):
        q_out[i, 0] = turned[:HEAD_DIM]
        q_out[i, 1] = turned[HEAD_DIM:]
    qw_out[...] = dot(normed, ready(3)).astype(bf16)


def stick_kernel(bias, q, kv, out, weight, keys, values):
    row = lax.axis_index("z")
    duo = lax.axis_index("yy")
    shift = jnp.where(lax.axis_index("hy") == 0, bias[0], bias[1]) * LOG2E
    blocks = kv.shape[0]
    pair = 2 * TILE
    r_i = lax.broadcasted_iota(jnp.int32, (pair, pair), 0)
    c_i = lax.broadcasted_iota(jnp.int32, (pair, pair), 1)
    after = jnp.where(c_i > r_i, 1.0, 0.0).astype(bf16)
    for j in range(blocks):
        cols = slice(j * TILE, (j + 1) * TILE)
        keys[cols] = kv[j, :, :HEAD_DIM]
        values[:, cols] = jnp.transpose(kv[j].astype(f32))[HEAD_DIM:].astype(bf16)

    def clear(block, _):
        out[2 * block] = jnp.zeros(out.shape[1:], bf16)
        out[2 * block + 1] = jnp.zeros(out.shape[1:], bf16)
        return 0

    lax.fori_loop(0, row, clear, 0)

    def block_step(block, masked):
        query = jnp.concatenate([q[2 * block], q[2 * block + 1]], axis=1)
        carry = [jnp.zeros((1, pair), f32)]

        def open_tile(j):
            s = dot(keys[j * TILE : (j + 2) * TILE], query) * (SCALE * LOG2E) + shift
            soft = jnp.maximum(s, lax.log2(1.0 + jnp.exp2(jnp.minimum(s, 126.0))))
            rest = s - soft
            if masked:
                seen = (j * TILE + r_i) < (duo * pair + c_i)
                soft = jnp.where(seen, soft, 0.0)
                rest = jnp.where(seen, rest, -jnp.inf)
            return rest, soft[:1], dot(after, soft.astype(bf16))

        def close_tile(j, rest, own, sums):
            w = jnp.exp2(rest - (sums + carry[0]))
            weight[j * TILE : (j + 2) * TILE] = w.astype(bf16)
            carry[0] = carry[0] + (sums[:1] + own)

        units = list(reversed(range(0, blocks, 2)))
        opened = open_tile(units[0])
        for at, unit in enumerate(units):
            following = open_tile(units[at + 1]) if at + 1 < len(units) else None
            close_tile(unit, *opened)
            opened = following
        acc = dot(values[...], weight[...])
        high, low = split(carry[0])
        tail = lax.broadcasted_iota(jnp.int32, (TAIL, pair), 0)
        tail = jnp.where(tail == 0, high.astype(f32), jnp.where(tail == 1, low.astype(f32), 0.0))
        for i in range(2):
            cols = slice(i * TILE, (i + 1) * TILE)
            out[2 * block + i, :HEAD_DIM] = acc[:, cols].astype(bf16)
            out[2 * block + i, HEAD_DIM:] = tail[:, cols].astype(bf16)

    block_step(row, True)

    def later(block, _):
        block_step(block, False)
        return 0

    lax.fori_loop(row + 1, out.shape[0] // 2, later, 0)


def window_kernel(sinks, qw, prev, own, w_out, gain, prod_out, ssq_out):
    lane = lax.broadcasted_iota(jnp.int32, (TILE, TILE), 1)
    first = lane < HEAD_DIM
    block = lax.axis_index("z") + lax.axis_index("yy") + lax.axis_index("hy")
    query = qw[...].astype(f32)
    both = jnp.concatenate(
        [jnp.where(first, query, 0.0), jnp.where(first, pltpu.roll(query, HEAD_DIM, 1), 0.0)], axis=0
    ).astype(bf16)
    pair = jnp.concatenate([prev[...], own[...]], axis=0)
    logits = dot(both, pair, 1, 1) * SCALE
    r_i = lax.broadcasted_iota(jnp.int32, (2 * TILE, 2 * TILE), 0)
    c_i = lax.broadcasted_iota(jnp.int32, (2 * TILE, 2 * TILE), 1)
    distance = r_i % TILE + WINDOW - c_i
    usable = (distance >= 0) & (distance < WINDOW) & (c_i >= TILE * jnp.where(block > 0, 0, 1))
    logits = jnp.where(usable, logits, -jnp.inf)
    sink = jnp.where(r_i[:, :1] < TILE, sinks[0], sinks[1])
    top = jnp.maximum(jnp.max(logits, axis=1, keepdims=True), sink)
    powers = jnp.exp(logits - top)
    total = jnp.sum(powers, axis=1, keepdims=True) + jnp.exp(sink - top)
    weights = (powers / total).astype(bf16)
    mixed = dot(weights, pair)
    result = jnp.where(first, pltpu.roll(mixed[:TILE], HEAD_DIM, 1), mixed[TILE:]).astype(bf16).astype(f32)
    ssq_out[...] = jnp.broadcast_to(jnp.sum(result * result, axis=1, keepdims=True), (TILE, TILE))
    scaled = (result * gain[...]).astype(bf16)
    prod_out[...] = dot(scaled, w_out[...]).astype(bf16)


def combine_kernel(parts, gain, w_out, prod_w, ssq_w, out):
    count = parts.shape[0] // 2
    width = w_out.shape[1]
    lane = lax.broadcasted_iota(jnp.int32, (TILE, TILE), 1)
    heads = []
    for h in range(2):
        later = jnp.zeros((1, TILE), f32)
        total = jnp.zeros((HEAD_DIM, TILE), f32)
        for z in reversed(range(count)):
            at = 2 * z + h
            total = total + parts[at, :HEAD_DIM].astype(f32) * jnp.exp2(-later)
            tail = parts[at, HEAD_DIM:].astype(f32)
            later = later + tail[0:1] + tail[1:2]
        heads.append(total)
    result = jnp.transpose(jnp.concatenate(heads, axis=0))
    result = result.astype(bf16).astype(f32)
    ssq = jnp.sum(result * result, axis=1, keepdims=True)
    scaled = (result * gain[...]).astype(bf16)
    out[:, :width] = dot(scaled, w_out[...]).astype(bf16)
    out[:, width : 2 * width] = prod_w[...]
    high_s, low_s = split(jnp.broadcast_to(ssq, (TILE, TILE)))
    high_w, low_w = split(ssq_w[...])
    out[:, 2 * width :] = jnp.where(
        lane == 0,
        high_s.astype(f32),
        jnp.where(lane == 1, low_s.astype(f32), jnp.where(lane == 2, high_w.astype(f32), low_w.astype(f32))),
    ).astype(bf16)


def final_kernel(parts, gain, out):
    width = out.shape[1]
    count = parts.shape[0]
    squares = sum(parts[i, :, 2 * width :].astype(f32) for i in range(count))
    stick = lax.rsqrt((squares[:, 0:1] + squares[:, 1:2]) / SB_WIDTH + epsilon)
    window = lax.rsqrt((squares[:, 2:3] + squares[:, 3:4]) / SW_WIDTH + epsilon)
    sum_s = sum(parts[i, :, :width].astype(f32) for i in range(count))
    sum_w = sum(parts[i, :, width : 2 * width].astype(f32) for i in range(count))
    combined = (sum_s * stick + sum_w * window).astype(bf16).astype(f32)
    mean = jnp.mean(combined * combined, axis=1, keepdims=True)
    out[...] = (combined * lax.rsqrt(mean + epsilon) * gain[...]).astype(bf16)


def shards(
    tokens,
    pre_gain,
    w_query_stick,
    w_key_stick,
    w_value_stick,
    w_query_window,
    w_key_window,
    w_value_window,
    stick_bias,
    sinks,
    stick_gain,
    window_gain,
    w_out_stick,
    w_out_window,
    post_gain,
):
    tok_rows, feats = tokens.shape
    nz, ntp = lax.axis_size("z"), lax.axis_size("tp")
    width = ntp * feats

    def swap(value, axis):
        return lax.all_to_all(value, axis, 0, 0, tiled=True)

    gathered = lax.all_gather(tokens, "tp", axis=0, tiled=True).reshape(ntp, tok_rows, feats)
    head_pair = w_key_stick.shape[1]

    def holders(arrays):
        return [pltpu.VMEM(a.shape, a.dtype) for a in arrays] + [pltpu.SemaphoreType.DMA((PIECES * len(arrays),))]

    weights = (w_key_stick, w_value_stick)
    gain = pre_gain.reshape(1, width)
    kv_all, normed = call(
        keys_kernel,
        (
            jax.ShapeDtypeStruct((ROWS, tok_rows, head_pair), bf16),
            jax.ShapeDtypeStruct((tok_rows, width), bf16),
        ),
        [VM, HB, HB, HB],
        scratch=holders(weights + (gain,)),
    )(gathered, gain, *weights)
    kv_row = swap(kv_all, ("yy", "hy"))
    weights = (w_query_stick, w_query_window, w_key_window.T, w_value_window.T)
    q_all, q_win, kv_win = call(
        rest_kernel,
        (
            jax.ShapeDtypeStruct((nz, 2, HEAD_DIM, tok_rows), bf16),
            jax.ShapeDtypeStruct((tok_rows, head_pair), bf16),
            jax.ShapeDtypeStruct((tok_rows, head_pair), bf16),
        ),
        [VM] + [HB] * 4,
        scratch=holders((weights[2], weights[3], weights[0], weights[1])),
    )(normed, *weights)
    count = nz * ROWS
    previous = lax.ppermute(kv_win, ("z", "yy", "hy"), [(i, i + 1) for i in range(count - 1)])
    q_col = swap(q_all.reshape(2 * nz, HEAD_DIM, tok_rows), ("z", "hy"))
    prod_w, ssq_w = call(
        window_kernel,
        (jax.ShapeDtypeStruct((tok_rows, width), bf16), jax.ShapeDtypeStruct((tok_rows, TILE), f32)),
        [SM] + [VM] * 5,
    )(sinks, q_win, previous, kv_win, w_out_window, window_gain.reshape(1, -1))
    partial = call(
        stick_kernel,
        jax.ShapeDtypeStruct((2 * nz, HEAD_DIM + TAIL, TILE), bf16),
        [SM, VM, VM],
        scratch=[
            pltpu.VMEM((ROWS * TILE, 2 * TILE), bf16),
            pltpu.VMEM((ROWS * TILE, HEAD_DIM), bf16),
            pltpu.VMEM((HEAD_DIM, ROWS * TILE), bf16),
        ],
    )(stick_bias, q_col, kv_row)
    returned = swap(partial, ("z", "hy"))
    sending = call(
        combine_kernel, jax.ShapeDtypeStruct((tok_rows, 2 * width + TILE), bf16), [VM] * 5
    )(returned, stick_gain.reshape(1, -1), w_out_stick, prod_w, ssq_w)
    arrived = swap(sending.reshape(ntp, tok_rows // ntp, 2 * width + TILE), "tp")
    return call(
        final_kernel, jax.ShapeDtypeStruct((tok_rows // ntp, width), bf16), [VM, VM], keep=False
    )(arrived, post_gain.reshape(1, width))


def solution(mesh):
    cube = Mesh(mesh.devices.reshape(-1, ROWS // 2, 2, mesh.devices.shape[-1]), ("z", "yy", "hy", "tp"))
    seq = ("z", "yy", "hy")
    in_specs = (
        P(seq, "tp"),
        P(),
        P(None, "tp"),
        P(None, "tp"),
        P(None, "tp"),
        P(None, "tp"),
        P(None, "tp"),
        P(None, "tp"),
        P("tp"),
        P("tp"),
        P("tp"),
        P("tp"),
        P("tp", None),
        P("tp", None),
        P(),
    )
    out_specs = P((*seq, "tp"), None)
    return jax.shard_map(shards, mesh=cube, in_specs=in_specs, out_specs=out_specs, check_vma=False)
```

```python
import jax
import jax.numpy as jnp
from jax import lax
from jax.experimental import pallas as pl
from jax.experimental.pallas import tpu as pltpu
from jax.sharding import Mesh, PartitionSpec as P


HEAD_DIM = 64
WINDOW = 128
TILE = 128
SB_WIDTH = 1024
SW_WIDTH = 1024
ROWS = 8
TAIL = 8
PIECES = 1
LOG2E = 1.4426950408889634
SCALE = HEAD_DIM ** (-0.5)

epsilon = 1e-06
f32 = jnp.float32
bf16 = jnp.bfloat16

VM = pl.BlockSpec(memory_space=pltpu.VMEM)
SM = pl.BlockSpec(memory_space=pltpu.SMEM)
HB = pl.BlockSpec(memory_space=pltpu.HBM)


def call(kernel, out_shape, in_specs, scratch=(), keep=True):
    many = isinstance(out_shape, (tuple, list))
    shapes = out_shape if many else [out_shape]
    if keep:
        shapes = [pltpu.VMEM(s.shape, s.dtype) for s in shapes]
    run = pl.pallas_call(
        kernel,
        out_shape=shapes if many else shapes[0],
        in_specs=in_specs,
        out_specs=[VM] * len(shapes) if many else VM,
        scratch_shapes=list(scratch),
        compiler_params=pltpu.CompilerParams(vmem_limit_bytes=16 * 2**20),
    )

    def begun(*args):
        spaces = {id(VM): pltpu.VMEM, id(HB): pltpu.HBM}
        return run(
            *[
                pltpu.with_memory_space_constraint(a, spaces[id(spec)]) if id(spec) in spaces else a
                for a, spec in zip(args, in_specs)
            ]
        )

    return begun


def dot(a, b, ca=1, cb=0):
    return lax.dot_general(a, b, (((ca,), (cb,)), ((), ())), preferred_element_type=f32)


def split(value):
    high = value.astype(bf16)
    return high, (value - high.astype(f32)).astype(bf16)


def fetched(sources, holders, sems):
    copies = []
    for source, holder in zip(sources, holders):
        step = source.shape[0] // PIECES if source.shape[0] % (8 * PIECES) == 0 else source.shape[0]
        copies.append([])
        for at in range(0, source.shape[0], step):
            piece = pl.ds(at, step)
            number = sum(map(len, copies))
            copies[-1].append(pltpu.make_async_copy(source.at[piece], holder.at[piece], sems.at[number]))
    for copy in sum(copies, []):
        copy.start()

    def ready(at):
        for copy in copies[at]:
            copy.wait()
        return holders[at][...]

    return ready


def keys_kernel(tok, gain, wk, wv, kv_out, normed_out, both, gains, sems):
    half = wk.shape[1]
    copies = [
        pltpu.make_async_copy(source, holder, sems.at[i])
        for i, (source, holder) in enumerate(
            ((gain, gains), (wk, both.at[:, :half]), (wv, both.at[:, half:]))
        )
    ]
    for copy in copies:
        copy.start()
    parts = tok.shape[0]
    wide = [tok[i].astype(f32) for i in range(parts)]
    total = sum(jnp.sum(w * w, axis=1, keepdims=True) for w in wide)
    scale = lax.rsqrt(total / (parts * tok.shape[2]) + epsilon)
    step = tok.shape[2]
    copies[0].wait()
    for i, w in enumerate(wide):
        normed_out[:, i * step : (i + 1) * step] = (w * scale * gains[:, i * step : (i + 1) * step]).astype(bf16)
    normed = normed_out[...]
    copies[1].wait()
    copies[2].wait()
    made = dot(normed, both[...])
    key, value = made[:, :half], made[:, half:]
    first = lax.broadcasted_iota(jnp.int32, (TILE, TILE), 1) < HEAD_DIM
    heads = [
        jnp.where(first, key, pltpu.roll(value, HEAD_DIM, 1)).astype(bf16),
        jnp.where(first, pltpu.roll(key, HEAD_DIM, 1), value).astype(bf16),
    ]
    for i in range(kv_out.shape[0]):
        kv_out[i] = heads[i % 2]


def rest_kernel(normed_in, wq, wqw, wkw, wvw, q_out, qw_out, kvw_out, *held):
    ready = fetched((wkw, wvw, wq, wqw), held[:4], held[4])
    normed = normed_in[...]
    kvw_out[:, :HEAD_DIM] = dot(normed, ready(0), 1, 1).astype(bf16)
    kvw_out[:, HEAD_DIM:] = dot(normed, ready(1), 1, 1).astype(bf16)
    query = dot(normed, ready(2)).astype(bf16)
    turned = jnp.transpose(query.astype(f32)).astype(bf16)
    for i in range(q_out.shape[0]):
        q_out[i, 0] = turned[:HEAD_DIM]
        q_out[i, 1] = turned[HEAD_DIM:]
    qw_out[...] = dot(normed, ready(3)).astype(bf16)


def stick_kernel(bias, q, kv, out, weight, keys, values):
    row = lax.axis_index("z")
    duo = lax.axis_index("yy")
    shift = jnp.where(lax.axis_index("hy") == 0, bias[0], bias[1]) * LOG2E
    blocks = kv.shape[0]
    pair = 2 * TILE
    r_i = lax.broadcasted_iota(jnp.int32, (pair, pair), 0)
    c_i = lax.broadcasted_iota(jnp.int32, (pair, pair), 1)
    after = jnp.where(c_i > r_i, 1.0, 0.0).astype(bf16)
    for j in range(blocks):
        cols = slice(j * TILE, (j + 1) * TILE)
        both = kv[j].astype(f32)
        high, low = split(both[:, :HEAD_DIM] * (SCALE * LOG2E))
        keys[cols, :HEAD_DIM] = high
        keys[cols, HEAD_DIM:] = low
        values[:, cols] = jnp.transpose(both)[HEAD_DIM:].astype(bf16)

    def clear(block, _):
        out[2 * block] = jnp.zeros(out.shape[1:], bf16)
        out[2 * block + 1] = jnp.zeros(out.shape[1:], bf16)
        return 0

    lax.fori_loop(0, row, clear, 0)

    def block_steps(steps):
        queries = [jnp.concatenate([q[2 * b], q[2 * b + 1]], axis=1) for b, _ in steps]
        queries = [jnp.concatenate([v, v], axis=0) for v in queries]
        carry = [jnp.zeros((1, pair), f32) for _ in steps]

        def open_tile(n, j):
            s = dot(keys[j * TILE : (j + 2) * TILE], queries[n]) + shift
            soft = jnp.maximum(s, lax.log2(1.0 + jnp.exp2(jnp.minimum(s, 126.0))))
            rest = s - soft
            if steps[n][1]:
                seen = (j * TILE + r_i) < (duo * pair + c_i)
                soft = jnp.where(seen, soft, 0.0)
                rest = jnp.where(seen, rest, -jnp.inf)
            return rest, soft[:1], dot(after, soft.astype(bf16))

        def close_tile(n, j, rest, own, sums):
            w = jnp.exp2(rest - (sums + carry[n]))
            weight[n, j * TILE : (j + 2) * TILE] = w.astype(bf16)
            carry[n] = carry[n] + (sums[:1] + own)

        units = [(n, j) for j in reversed(range(0, blocks, 2)) for n in range(len(steps))]
        opened = open_tile(*units[0])
        for at, unit in enumerate(units):
            following = open_tile(*units[at + 1]) if at + 1 < len(units) else None
            close_tile(*unit, *opened)
            opened = following
        for n in reversed(range(len(steps))):
            block = steps[n][0]
            acc = dot(values[...], weight[n])
            high, low = split(carry[n])
            tail = lax.broadcasted_iota(jnp.int32, (TAIL, pair), 0)
            tail = jnp.where(tail == 0, high.astype(f32), jnp.where(tail == 1, low.astype(f32), 0.0))
            for i in range(2):
                cols = slice(i * TILE, (i + 1) * TILE)
                out[2 * block + i, :HEAD_DIM] = acc[:, cols].astype(bf16)
                out[2 * block + i, HEAD_DIM:] = tail[:, cols].astype(bf16)

    last = out.shape[0] // 2 - 1
    block_steps(((row, True), (jnp.minimum(row + 1, last), False)))

    def later(step, _):
        block = row + 2 + 2 * step
        block_steps(((block, False), (jnp.minimum(block + 1, last), False)))
        return 0

    lax.fori_loop(0, lax.div(last - row, 2), later, 0)


def window_kernel(sinks, qw, prev, own, w_out, gain, prod_out, ssq_out):
    lane = lax.broadcasted_iota(jnp.int32, (TILE, TILE), 1)
    first = lane < HEAD_DIM
    block = lax.axis_index("z") + lax.axis_index("yy") + lax.axis_index("hy")
    query = qw[...].astype(f32)
    both = jnp.concatenate(
        [jnp.where(first, query, 0.0), jnp.where(first, pltpu.roll(query, HEAD_DIM, 1), 0.0)], axis=0
    ).astype(bf16)
    pair = jnp.concatenate([prev[...], own[...]], axis=0)
    logits = dot(both, pair, 1, 1) * SCALE
    r_i = lax.broadcasted_iota(jnp.int32, (2 * TILE, 2 * TILE), 0)
    c_i = lax.broadcasted_iota(jnp.int32, (2 * TILE, 2 * TILE), 1)
    distance = r_i % TILE + WINDOW - c_i
    usable = (distance >= 0) & (distance < WINDOW) & (c_i >= TILE * jnp.where(block > 0, 0, 1))
    logits = jnp.where(usable, logits, -jnp.inf)
    sink = jnp.where(r_i[:, :1] < TILE, sinks[0], sinks[1])
    top = jnp.maximum(jnp.max(logits, axis=1, keepdims=True), sink)
    powers = jnp.exp(logits - top)
    total = jnp.sum(powers, axis=1, keepdims=True) + jnp.exp(sink - top)
    weights = (powers / total).astype(bf16)
    mixed = dot(weights, pair)
    result = jnp.where(first, pltpu.roll(mixed[:TILE], HEAD_DIM, 1), mixed[TILE:]).astype(bf16).astype(f32)
    ssq_out[...] = jnp.broadcast_to(jnp.sum(result * result, axis=1, keepdims=True), (TILE, TILE))
    scaled = (result * gain[...]).astype(bf16)
    prod_out[...] = dot(scaled, w_out[...]).astype(bf16)


def combine_kernel(parts, gain, w_out, prod_w, ssq_w, out):
    count = parts.shape[0] // 2
    width = w_out.shape[1]
    lane = lax.broadcasted_iota(jnp.int32, (TILE, TILE), 1)
    heads = []
    for h in range(2):
        later = jnp.zeros((1, TILE), f32)
        total = jnp.zeros((HEAD_DIM, TILE), f32)
        for z in reversed(range(count)):
            at = 2 * z + h
            total = total + parts[at, :HEAD_DIM].astype(f32) * jnp.exp2(-later)
            tail = parts[at, HEAD_DIM:].astype(f32)
            later = later + tail[0:1] + tail[1:2]
        heads.append(total)
    result = jnp.transpose(jnp.concatenate(heads, axis=0))
    result = result.astype(bf16).astype(f32)
    ssq = jnp.sum(result * result, axis=1, keepdims=True)
    scaled = (result * gain[...]).astype(bf16)
    out[:, :width] = dot(scaled, w_out[...]).astype(bf16)
    out[:, width : 2 * width] = prod_w[...]
    high_s, low_s = split(jnp.broadcast_to(ssq, (TILE, TILE)))
    high_w, low_w = split(ssq_w[...])
    out[:, 2 * width :] = jnp.where(
        lane == 0,
        high_s.astype(f32),
        jnp.where(lane == 1, low_s.astype(f32), jnp.where(lane == 2, high_w.astype(f32), low_w.astype(f32))),
    ).astype(bf16)


def final_kernel(parts, gain, out):
    width = out.shape[1]
    count = parts.shape[0]
    squares = sum(parts[i, :, 2 * width :].astype(f32) for i in range(count))
    stick = lax.rsqrt((squares[:, 0:1] + squares[:, 1:2]) / SB_WIDTH + epsilon)
    window = lax.rsqrt((squares[:, 2:3] + squares[:, 3:4]) / SW_WIDTH + epsilon)
    sum_s = sum(parts[i, :, :width].astype(f32) for i in range(count))
    sum_w = sum(parts[i, :, width : 2 * width].astype(f32) for i in range(count))
    combined = (sum_s * stick + sum_w * window).astype(bf16).astype(f32)
    mean = jnp.mean(combined * combined, axis=1, keepdims=True)
    out[...] = (combined * lax.rsqrt(mean + epsilon) * gain[...]).astype(bf16)


def shards(
    tokens,
    pre_gain,
    w_query_stick,
    w_key_stick,
    w_value_stick,
    w_query_window,
    w_key_window,
    w_value_window,
    stick_bias,
    sinks,
    stick_gain,
    window_gain,
    w_out_stick,
    w_out_window,
    post_gain,
):
    tok_rows, feats = tokens.shape
    nz, ntp = lax.axis_size("z"), lax.axis_size("tp")
    width = ntp * feats

    def swap(value, axis):
        return lax.all_to_all(value, axis, 0, 0, tiled=True)

    gathered = lax.all_gather(tokens, "tp", axis=0, tiled=True).reshape(ntp, tok_rows, feats)
    head_pair = w_key_stick.shape[1]

    def holders(arrays):
        return [pltpu.VMEM(a.shape, a.dtype) for a in arrays] + [pltpu.SemaphoreType.DMA((PIECES * len(arrays),))]

    gain = pre_gain.reshape(1, width)
    kv_all, normed = call(
        keys_kernel,
        (
            jax.ShapeDtypeStruct((ROWS, tok_rows, head_pair), bf16),
            jax.ShapeDtypeStruct((tok_rows, width), bf16),
        ),
        [VM, HB, HB, HB],
        scratch=[
            pltpu.VMEM((width, 2 * head_pair), bf16),
            pltpu.VMEM((1, width), f32),
            pltpu.SemaphoreType.DMA((3,)),
        ],
    )(gathered, gain, w_key_stick, w_value_stick)
    kv_row = swap(kv_all, ("yy", "hy"))
    weights = (w_query_stick, w_query_window, w_key_window.T, w_value_window.T)
    q_all, q_win, kv_win = call(
        rest_kernel,
        (
            jax.ShapeDtypeStruct((nz, 2, HEAD_DIM, tok_rows), bf16),
            jax.ShapeDtypeStruct((tok_rows, head_pair), bf16),
            jax.ShapeDtypeStruct((tok_rows, head_pair), bf16),
        ),
        [VM] + [HB] * 4,
        scratch=holders((weights[2], weights[3], weights[0], weights[1])),
    )(normed, *weights)
    count = nz * ROWS
    previous = lax.ppermute(kv_win, ("z", "yy", "hy"), [(i, i + 1) for i in range(count - 1)])
    q_col = swap(q_all.reshape(2 * nz, HEAD_DIM, tok_rows), ("z", "hy"))
    prod_w, ssq_w = call(
        window_kernel,
        (jax.ShapeDtypeStruct((tok_rows, width), bf16), jax.ShapeDtypeStruct((tok_rows, TILE), f32)),
        [SM] + [VM] * 5,
    )(sinks, q_win, previous, kv_win, w_out_window, window_gain.reshape(1, -1))
    partial = call(
        stick_kernel,
        jax.ShapeDtypeStruct((2 * nz, HEAD_DIM + TAIL, TILE), bf16),
        [SM, VM, VM],
        scratch=[
            pltpu.VMEM((2, ROWS * TILE, 2 * TILE), bf16),
            pltpu.VMEM((ROWS * TILE, 2 * HEAD_DIM), bf16),
            pltpu.VMEM((HEAD_DIM, ROWS * TILE), bf16),
        ],
    )(stick_bias, q_col, kv_row)
    returned = swap(partial, ("z", "hy"))
    sending = call(
        combine_kernel, jax.ShapeDtypeStruct((tok_rows, 2 * width + TILE), bf16), [VM] * 5
    )(returned, stick_gain.reshape(1, -1), w_out_stick, prod_w, ssq_w)
    arrived = swap(sending.reshape(ntp, tok_rows // ntp, 2 * width + TILE), "tp")
    return call(
        final_kernel, jax.ShapeDtypeStruct((tok_rows // ntp, width), bf16), [VM, VM], keep=False
    )(arrived, post_gain.reshape(1, width))


def solution(mesh):
    cube = Mesh(mesh.devices.reshape(-1, ROWS // 2, 2, mesh.devices.shape[-1]), ("z", "yy", "hy", "tp"))
    seq = ("z", "yy", "hy")
    in_specs = (
        P(seq, "tp"),
        P(),
        P(None, "tp"),
        P(None, "tp"),
        P(None, "tp"),
        P(None, "tp"),
        P(None, "tp"),
        P(None, "tp"),
        P("tp"),
        P("tp"),
        P("tp"),
        P("tp"),
        P("tp", None),
        P("tp", None),
        P(),
    )
    out_specs = P((*seq, "tp"), None)
    return jax.shard_map(shards, mesh=cube, in_specs=in_specs, out_specs=out_specs, check_vma=False)
```

```python
import jax
import jax.numpy as jnp
from jax import lax
from jax.experimental import pallas as pl
from jax.experimental.pallas import tpu as pltpu
from jax.sharding import Mesh, PartitionSpec as P


HEAD_DIM = 64
WINDOW = 128
TILE = 128
SB_WIDTH = 1024
SW_WIDTH = 1024
ROWS = 8
TAIL = 8
PIECES = 1
LOG2E = 1.4426950408889634
SCALE = HEAD_DIM ** (-0.5)

epsilon = 1e-06
TP = ("x", "core")
f32 = jnp.float32
bf16 = jnp.bfloat16

VM = pl.BlockSpec(memory_space=pltpu.VMEM)
SM = pl.BlockSpec(memory_space=pltpu.SMEM)
HB = pl.BlockSpec(memory_space=pltpu.HBM)


def call(kernel, out_shape, in_specs, scratch=(), keep=True):
    many = isinstance(out_shape, (tuple, list))
    shapes = out_shape if many else [out_shape]
    if keep:
        shapes = [pltpu.VMEM(s.shape, s.dtype) for s in shapes]
    run = pl.pallas_call(
        kernel,
        out_shape=shapes if many else shapes[0],
        in_specs=in_specs,
        out_specs=[VM] * len(shapes) if many else VM,
        scratch_shapes=list(scratch),
        compiler_params=pltpu.CompilerParams(vmem_limit_bytes=16 * 2**20),
    )

    def begun(*args):
        spaces = {id(VM): pltpu.VMEM, id(HB): pltpu.HBM}
        return run(
            *[
                pltpu.with_memory_space_constraint(a, spaces[id(spec)]) if id(spec) in spaces else a
                for a, spec in zip(args, in_specs)
            ]
        )

    return begun


def dot(a, b, ca=1, cb=0):
    return lax.dot_general(a, b, (((ca,), (cb,)), ((), ())), preferred_element_type=f32)


def split(value):
    high = value.astype(bf16)
    return high, (value - high.astype(f32)).astype(bf16)


def fetched(sources, holders, sems):
    copies = []
    for source, holder in zip(sources, holders):
        step = source.shape[0] // PIECES if source.shape[0] % (8 * PIECES) == 0 else source.shape[0]
        copies.append([])
        for at in range(0, source.shape[0], step):
            piece = pl.ds(at, step)
            number = sum(map(len, copies))
            copies[-1].append(pltpu.make_async_copy(source.at[piece], holder.at[piece], sems.at[number]))
    for copy in sum(copies, []):
        copy.start()

    def ready(at):
        for copy in copies[at]:
            copy.wait()
        return holders[at][...]

    return ready


def keys_kernel(tok, gain, wk, wv, kv_out, normed_out, both, gains, sems):
    half = wk.shape[1]
    copies = [
        pltpu.make_async_copy(source, holder, sems.at[i])
        for i, (source, holder) in enumerate(
            ((gain, gains), (wk, both.at[:, :half]), (wv, both.at[:, half:]))
        )
    ]
    for copy in copies:
        copy.start()
    parts = tok.shape[0]
    wide = [tok[i].astype(f32) for i in range(parts)]
    total = sum(jnp.sum(w * w, axis=1, keepdims=True) for w in wide)
    scale = lax.rsqrt(total / (parts * tok.shape[2]) + epsilon)
    step = tok.shape[2]
    copies[0].wait()
    for i, w in enumerate(wide):
        normed_out[:, i * step : (i + 1) * step] = (w * scale * gains[:, i * step : (i + 1) * step]).astype(bf16)
    normed = normed_out[...]
    copies[1].wait()
    copies[2].wait()
    made = dot(normed, both[...])
    key, value = made[:, :half], made[:, half:]
    first = lax.broadcasted_iota(jnp.int32, (TILE, TILE), 1) < HEAD_DIM
    heads = [
        jnp.where(first, key, pltpu.roll(value, HEAD_DIM, 1)).astype(bf16),
        jnp.where(first, pltpu.roll(key, HEAD_DIM, 1), value).astype(bf16),
    ]
    for i in range(kv_out.shape[0]):
        kv_out[i] = heads[i % 2]


def rest_kernel(normed_in, wq, wqw, wkw, wvw, q_out, qw_out, kvw_out, *held):
    ready = fetched((wkw, wvw, wq, wqw), held[:4], held[4])
    normed = normed_in[...]
    kvw_out[:, :HEAD_DIM] = dot(normed, ready(0), 1, 1).astype(bf16)
    kvw_out[:, HEAD_DIM:] = dot(normed, ready(1), 1, 1).astype(bf16)
    query = dot(normed, ready(2)).astype(bf16)
    turned = jnp.transpose(query.astype(f32)).astype(bf16)
    for i in range(q_out.shape[0]):
        q_out[i, 0] = turned[:HEAD_DIM]
        q_out[i, 1] = turned[HEAD_DIM:]
    qw_out[...] = dot(normed, ready(3)).astype(bf16)


def stick_kernel(bias, q, kv, out, weight, keys, values):
    row = lax.axis_index("z")
    duo = lax.axis_index("yy")
    shift = jnp.where(lax.axis_index("hy") == 0, bias[0], bias[1]) * LOG2E
    blocks = kv.shape[0]
    pair = 2 * TILE
    r_i = lax.broadcasted_iota(jnp.int32, (pair, pair), 0)
    c_i = lax.broadcasted_iota(jnp.int32, (pair, pair), 1)
    after = jnp.where(c_i > r_i, 1.0, 0.0).astype(bf16)
    for j in range(blocks):
        cols = slice(j * TILE, (j + 1) * TILE)
        both = kv[j].astype(f32)
        high, low = split(both[:, :HEAD_DIM] * (SCALE * LOG2E))
        keys[cols, :HEAD_DIM] = high
        keys[cols, HEAD_DIM:] = low
        values[:, cols] = jnp.transpose(both)[HEAD_DIM:].astype(bf16)

    def clear(block, _):
        out[2 * block] = jnp.zeros(out.shape[1:], bf16)
        out[2 * block + 1] = jnp.zeros(out.shape[1:], bf16)
        return 0

    lax.fori_loop(0, row, clear, 0)

    def block_steps(steps):
        queries = [jnp.concatenate([q[2 * b], q[2 * b + 1]], axis=1) for b, _ in steps]
        queries = [jnp.concatenate([v, v], axis=0) for v in queries]
        carry = [jnp.zeros((1, pair), f32) for _ in steps]

        def open_tile(n, j):
            s = dot(keys[j * TILE : (j + 2) * TILE], queries[n]) + shift
            soft = jnp.maximum(s, lax.log2(1.0 + jnp.exp2(jnp.minimum(s, 126.0))))
            rest = s - soft
            if steps[n][1]:
                seen = (j * TILE + r_i) < (duo * pair + c_i)
                soft = jnp.where(seen, soft, 0.0)
                rest = jnp.where(seen, rest, -jnp.inf)
            return rest, soft[:1], dot(after, soft.astype(bf16))

        def close_tile(n, j, rest, own, sums):
            w = jnp.exp2(rest - (sums + carry[n]))
            weight[n, j * TILE : (j + 2) * TILE] = w.astype(bf16)
            carry[n] = carry[n] + (sums[:1] + own)

        units = [(n, j) for j in reversed(range(0, blocks, 2)) for n in range(len(steps))]
        opened = open_tile(*units[0])
        for at, unit in enumerate(units):
            following = open_tile(*units[at + 1]) if at + 1 < len(units) else None
            close_tile(*unit, *opened)
            opened = following
        for n in reversed(range(len(steps))):
            block = steps[n][0]
            acc = dot(values[...], weight[n])
            high, low = split(carry[n])
            tail = lax.broadcasted_iota(jnp.int32, (TAIL, pair), 0)
            tail = jnp.where(tail == 0, high.astype(f32), jnp.where(tail == 1, low.astype(f32), 0.0))
            for i in range(2):
                cols = slice(i * TILE, (i + 1) * TILE)
                out[2 * block + i, :HEAD_DIM] = acc[:, cols].astype(bf16)
                out[2 * block + i, HEAD_DIM:] = tail[:, cols].astype(bf16)

    last = out.shape[0] // 2 - 1
    block_steps(((row, True), (jnp.minimum(row + 1, last), False)))

    def later(step, _):
        block = row + 2 + 2 * step
        block_steps(((block, False), (jnp.minimum(block + 1, last), False)))
        return 0

    lax.fori_loop(0, lax.div(last - row, 2), later, 0)


def window_kernel(sinks, qw, prev, own, w_out, gain, keep, send):
    lane = lax.broadcasted_iota(jnp.int32, (TILE, TILE), 1)
    first = lane < HEAD_DIM
    block = lax.axis_index("z") + lax.axis_index("yy") + lax.axis_index("hy")
    query = qw[...].astype(f32)
    both = jnp.concatenate(
        [jnp.where(first, query, 0.0), jnp.where(first, pltpu.roll(query, HEAD_DIM, 1), 0.0)], axis=0
    ).astype(bf16)
    pair = jnp.concatenate([prev[...], own[...]], axis=0)
    logits = dot(both, pair, 1, 1) * SCALE
    r_i = lax.broadcasted_iota(jnp.int32, (2 * TILE, 2 * TILE), 0)
    c_i = lax.broadcasted_iota(jnp.int32, (2 * TILE, 2 * TILE), 1)
    distance = r_i % TILE + WINDOW - c_i
    usable = (distance >= 0) & (distance < WINDOW) & (c_i >= TILE * jnp.where(block > 0, 0, 1))
    logits = jnp.where(usable, logits, -jnp.inf)
    sink = jnp.where(r_i[:, :1] < TILE, sinks[0], sinks[1])
    top = jnp.maximum(jnp.max(logits, axis=1, keepdims=True), sink)
    powers = jnp.exp(logits - top)
    total = jnp.sum(powers, axis=1, keepdims=True) + jnp.exp(sink - top)
    weights = (powers / total).astype(bf16)
    mixed = dot(weights, pair)
    result = jnp.where(first, pltpu.roll(mixed[:TILE], HEAD_DIM, 1), mixed[TILE:]).astype(bf16).astype(f32)
    share(result, gain, w_out, keep, send)


def share(result, gain, w_out, keep, send):
    width = w_out.shape[1]
    ssq = jnp.sum(result * result, axis=1, keepdims=True)
    high, low = split(jnp.broadcast_to(ssq, (TILE, TILE)))
    lane = lax.broadcasted_iota(jnp.int32, (TILE, TILE), 1)
    squares = jnp.where(lane == 0, high.astype(f32), low.astype(f32))
    product = dot((result * gain[...]).astype(bf16), w_out[...])
    own = lax.axis_index("core") == 0
    rows = keep.shape[1]
    for value, cols in ((product, slice(0, width)), (squares, slice(width, width + TILE))):
        for at in range(keep.shape[0]):
            even = value[2 * at * rows : (2 * at + 1) * rows]
            odd = value[(2 * at + 1) * rows : (2 * at + 2) * rows]
            keep[at, :, cols] = jnp.where(own, even, odd).astype(bf16)
            send[at, :, cols] = jnp.where(own, odd, even).astype(bf16)


def combine_kernel(parts, gain, w_out, keep, send):
    count = parts.shape[0] // 2
    heads = []
    for h in range(2):
        later = jnp.zeros((1, TILE), f32)
        total = jnp.zeros((HEAD_DIM, TILE), f32)
        for z in reversed(range(count)):
            at = 2 * z + h
            total = total + parts[at, :HEAD_DIM].astype(f32) * jnp.exp2(-later)
            tail = parts[at, HEAD_DIM:].astype(f32)
            later = later + tail[0:1] + tail[1:2]
        heads.append(total)
    result = jnp.transpose(jnp.concatenate(heads, axis=0))
    share(result.astype(bf16).astype(f32), gain, w_out, keep, send)


def pairs_kernel(keep_s, came_s, keep_w, came_w, out):
    width = keep_s.shape[2] - TILE
    lane = lax.broadcasted_iota(jnp.int32, (keep_s.shape[1], TILE), 1)
    for at in range(out.shape[0]):
        parts = []
        for n, (keep, came) in enumerate(((keep_s, came_s), (keep_w, came_w))):
            both = keep[at].astype(f32) + came[at].astype(f32)
            out[at, :, n * width : (n + 1) * width] = both[:, :width].astype(bf16)
            parts += split(both[:, width : width + 1] + both[:, width + 1 : width + 2])
        tail = parts[-1].astype(f32)
        for n in reversed(range(len(parts) - 1)):
            tail = jnp.where(lane == n, parts[n].astype(f32), tail)
        out[at, :, 2 * width :] = tail.astype(bf16)


def final_kernel(parts, gain, out):
    width = out.shape[1]
    count = parts.shape[0]
    squares = sum(parts[i, :, 2 * width :].astype(f32) for i in range(count))
    stick = lax.rsqrt((squares[:, 0:1] + squares[:, 1:2]) / SB_WIDTH + epsilon)
    window = lax.rsqrt((squares[:, 2:3] + squares[:, 3:4]) / SW_WIDTH + epsilon)
    sum_s = sum(parts[i, :, :width].astype(f32) for i in range(count))
    sum_w = sum(parts[i, :, width : 2 * width].astype(f32) for i in range(count))
    combined = (sum_s * stick + sum_w * window).astype(bf16).astype(f32)
    mean = jnp.mean(combined * combined, axis=1, keepdims=True)
    out[...] = (combined * lax.rsqrt(mean + epsilon) * gain[...]).astype(bf16)


def shards(
    tokens,
    pre_gain,
    w_query_stick,
    w_key_stick,
    w_value_stick,
    w_query_window,
    w_key_window,
    w_value_window,
    stick_bias,
    sinks,
    stick_gain,
    window_gain,
    w_out_stick,
    w_out_window,
    post_gain,
):
    tok_rows, feats = tokens.shape
    nz, ntp = lax.axis_size("z"), lax.axis_size(TP)
    width = ntp * feats

    def swap(value, axis):
        return lax.all_to_all(value, axis, 0, 0, tiled=True)

    gathered = lax.all_gather(tokens, TP, axis=0, tiled=True).reshape(ntp, tok_rows, feats)
    head_pair = w_key_stick.shape[1]

    def holders(arrays):
        return [pltpu.VMEM(a.shape, a.dtype) for a in arrays] + [pltpu.SemaphoreType.DMA((PIECES * len(arrays),))]

    gain = pre_gain.reshape(1, width)
    kv_all, normed = call(
        keys_kernel,
        (
            jax.ShapeDtypeStruct((ROWS, tok_rows, head_pair), bf16),
            jax.ShapeDtypeStruct((tok_rows, width), bf16),
        ),
        [VM, HB, HB, HB],
        scratch=[
            pltpu.VMEM((width, 2 * head_pair), bf16),
            pltpu.VMEM((1, width), f32),
            pltpu.SemaphoreType.DMA((3,)),
        ],
    )(gathered, gain, w_key_stick, w_value_stick)
    kv_row = swap(kv_all, ("yy", "hy"))
    weights = (w_query_stick, w_query_window, w_key_window.T, w_value_window.T)
    q_all, q_win, kv_win = call(
        rest_kernel,
        (
            jax.ShapeDtypeStruct((nz, 2, HEAD_DIM, tok_rows), bf16),
            jax.ShapeDtypeStruct((tok_rows, head_pair), bf16),
            jax.ShapeDtypeStruct((tok_rows, head_pair), bf16),
        ),
        [VM] + [HB] * 4,
        scratch=holders((weights[2], weights[3], weights[0], weights[1])),
    )(normed, *weights)
    count = nz * ROWS
    previous = lax.ppermute(kv_win, ("z", "yy", "hy"), [(i, i + 1) for i in range(count - 1)])
    q_col = swap(q_all.reshape(2 * nz, HEAD_DIM, tok_rows), ("z", "hy"))
    rows = tok_rows // ntp
    halves = (jax.ShapeDtypeStruct((ntp // 2, rows, width + TILE), bf16),) * 2
    keep_w, send_w = call(window_kernel, halves, [SM] + [VM] * 5)(
        sinks, q_win, previous, kv_win, w_out_window, window_gain.reshape(1, -1)
    )

    def to_other_core(value):
        return lax.ppermute(value, "core", [(0, 1), (1, 0)])

    came_w = to_other_core(send_w)
    partial = call(
        stick_kernel,
        jax.ShapeDtypeStruct((2 * nz, HEAD_DIM + TAIL, TILE), bf16),
        [SM, VM, VM],
        scratch=[
            pltpu.VMEM((2, ROWS * TILE, 2 * TILE), bf16),
            pltpu.VMEM((ROWS * TILE, 2 * HEAD_DIM), bf16),
            pltpu.VMEM((HEAD_DIM, ROWS * TILE), bf16),
        ],
    )(stick_bias, q_col, kv_row)
    returned = swap(partial, ("z", "hy"))
    keep_s, send_s = call(combine_kernel, halves, [VM] * 3)(returned, stick_gain.reshape(1, -1), w_out_stick)
    came_s = to_other_core(send_s)
    sending = call(
        pairs_kernel, jax.ShapeDtypeStruct((ntp // 2, rows, 2 * width + TILE), bf16), [VM] * 4
    )(keep_s, came_s, keep_w, came_w)
    arrived = swap(sending, "x")
    return call(
        final_kernel, jax.ShapeDtypeStruct((rows, width), bf16), [VM, VM], keep=False
    )(arrived, post_gain.reshape(1, width))


def solution(mesh):
    cube = Mesh(
        mesh.devices.reshape(-1, ROWS // 2, 2, mesh.devices.shape[-1] // 2, 2), ("z", "yy", "hy", "x", "core")
    )
    seq = ("z", "yy", "hy")
    in_specs = (
        P(seq, TP),
        P(),
        P(None, TP),
        P(None, TP),
        P(None, TP),
        P(None, TP),
        P(None, TP),
        P(None, TP),
        P(TP),
        P(TP),
        P(TP),
        P(TP),
        P(TP, None),
        P(TP, None),
        P(),
    )
    out_specs = P((*seq, *TP), None)
    return jax.shard_map(shards, mesh=cube, in_specs=in_specs, out_specs=out_specs, check_vma=False)
```

```python
import jax
import jax.numpy as jnp
from jax import lax
from jax.experimental import pallas as pl
from jax.experimental.pallas import tpu as pltpu
from jax.sharding import Mesh, PartitionSpec as P


HEAD_DIM = 64
WINDOW = 128
TILE = 128
SB_WIDTH = 1024
SW_WIDTH = 1024
ROWS = 8
TAIL = 8
LOG2E = 1.4426950408889634
SCALE = HEAD_DIM ** (-0.5)

epsilon = 1e-06
TP = ("x", "core")
f32 = jnp.float32
bf16 = jnp.bfloat16

VM = pl.BlockSpec(memory_space=pltpu.VMEM)
SM = pl.BlockSpec(memory_space=pltpu.SMEM)
HB = pl.BlockSpec(memory_space=pltpu.HBM)


def call(kernel, out_shape, in_specs, scratch=(), keep=True):
    many = isinstance(out_shape, (tuple, list))
    shapes = out_shape if many else [out_shape]
    if keep:
        shapes = [pltpu.VMEM(s.shape, s.dtype) for s in shapes]
    run = pl.pallas_call(
        kernel,
        out_shape=shapes if many else shapes[0],
        in_specs=in_specs,
        out_specs=[VM] * len(shapes) if many else VM,
        scratch_shapes=list(scratch),
        compiler_params=pltpu.CompilerParams(vmem_limit_bytes=16 * 2**20),
    )

    def begun(*args):
        spaces = {id(VM): pltpu.VMEM, id(HB): pltpu.HBM}
        return run(
            *[
                pltpu.with_memory_space_constraint(a, spaces[id(spec)]) if id(spec) in spaces else a
                for a, spec in zip(args, in_specs)
            ]
        )

    return begun


def dot(a, b, ca=1, cb=0):
    return lax.dot_general(a, b, (((ca,), (cb,)), ((), ())), preferred_element_type=f32)


def split(value):
    high = value.astype(bf16)
    return high, (value - high.astype(f32)).astype(bf16)


def fetched(sources, targets, sems):
    copies = [pltpu.make_async_copy(s, t, sems.at[i]) for i, (s, t) in enumerate(zip(sources, targets))]
    for copy in copies:
        copy.start()
    return lambda at: copies[at].wait()


def queries_kernel(tok, gain, wq, q_out, gained_out, scale_out, gains, held, sems):
    wait = fetched((gain, wq), (gains, held), sems)
    cores, chips, rows, step = tok.shape
    total = jnp.zeros((rows, step), f32)
    wait(0)
    for x in range(chips):
        for c in range(cores):
            w = tok[c, x].astype(f32)
            total = total + w * w
            cols = slice((x * cores + c) * step, (x * cores + c + 1) * step)
            gained_out[:, cols] = (w * gains[:, cols]).astype(bf16)
    wait(1)
    mean = jnp.sum(total, axis=1, keepdims=True) / (chips * cores * step)
    scale = jnp.broadcast_to(lax.rsqrt(mean + epsilon), (rows, TILE))
    scale_out[...] = scale
    query = (dot(gained_out[...], held[...]) * scale).astype(bf16)
    turned = jnp.transpose(query.astype(f32)).astype(bf16)
    for i in range(q_out.shape[0]):
        q_out[i, 0] = turned[:HEAD_DIM]
        q_out[i, 1] = turned[HEAD_DIM:]


def rest_kernel(gained_in, scale_in, wk, wv, wqw, wkw, wvw, kv_out, qw_out, kvw_out, both, held, narrow, sems):
    half = wk.shape[1]
    wait = fetched(
        (wk, wv, wqw, wkw, wvw),
        (both.at[:, :half], both.at[:, half:], held, narrow.at[:HEAD_DIM], narrow.at[HEAD_DIM:]),
        sems,
    )
    gained = gained_in[...]
    scale = scale_in[...]
    wait(3)
    wait(4)
    kvw_out[...] = (dot(gained, narrow[...], 1, 1) * scale).astype(bf16)
    wait(0)
    wait(1)
    made = dot(gained, both[...])
    key, value = made[:, :half] * scale, made[:, half:] * scale
    first = lax.broadcasted_iota(jnp.int32, (TILE, TILE), 1) < HEAD_DIM
    heads = [
        jnp.where(first, key, pltpu.roll(value, HEAD_DIM, 1)).astype(bf16),
        jnp.where(first, pltpu.roll(key, HEAD_DIM, 1), value).astype(bf16),
    ]
    for i in range(kv_out.shape[0]):
        kv_out[i] = heads[i % 2]
    wait(2)
    qw_out[...] = (dot(gained, held[...]) * scale).astype(bf16)


def stick_kernel(bias, q, kv, out, weight, keys, values):
    row = lax.axis_index("z")
    duo = lax.axis_index("yy")
    shift = jnp.where(lax.axis_index("hy") == 0, bias[0], bias[1]) * LOG2E
    blocks = kv.shape[0]
    pair = 2 * TILE
    r_i = lax.broadcasted_iota(jnp.int32, (pair, pair), 0)
    c_i = lax.broadcasted_iota(jnp.int32, (pair, pair), 1)
    after = jnp.where(c_i > r_i, 1.0, 0.0).astype(bf16)
    for j in range(blocks):
        cols = slice(j * TILE, (j + 1) * TILE)
        both = kv[j].astype(f32)
        high, low = split(both[:, :HEAD_DIM] * (SCALE * LOG2E))
        keys[cols, :HEAD_DIM] = high
        keys[cols, HEAD_DIM:] = low
        values[:, cols] = jnp.transpose(both)[HEAD_DIM:].astype(bf16)

    def clear(block, _):
        out[2 * block] = jnp.zeros(out.shape[1:], bf16)
        out[2 * block + 1] = jnp.zeros(out.shape[1:], bf16)
        return 0

    lax.fori_loop(0, row, clear, 0)

    def block_steps(steps):
        queries = [jnp.concatenate([q[2 * b], q[2 * b + 1]], axis=1) for b, _ in steps]
        queries = [jnp.concatenate([v, v], axis=0) for v in queries]
        carry = [jnp.zeros((1, pair), f32) for _ in steps]

        def open_tile(n, j):
            s = dot(keys[j * TILE : (j + 2) * TILE], queries[n]) + shift
            soft = jnp.maximum(s, lax.log2(1.0 + jnp.exp2(jnp.minimum(s, 126.0))))
            rest = s - soft
            if steps[n][1]:
                seen = (j * TILE + r_i) < (duo * pair + c_i)
                soft = jnp.where(seen, soft, 0.0)
                rest = jnp.where(seen, rest, -jnp.inf)
            return rest, soft[:1], dot(after, soft.astype(bf16))

        def close_tile(n, j, rest, own, sums):
            w = jnp.exp2(rest - (sums + carry[n]))
            weight[n, j * TILE : (j + 2) * TILE] = w.astype(bf16)
            carry[n] = carry[n] + (sums[:1] + own)

        units = [(n, j) for j in reversed(range(0, blocks, 2)) for n in range(len(steps))]
        opened = open_tile(*units[0])
        for at, unit in enumerate(units):
            following = open_tile(*units[at + 1]) if at + 1 < len(units) else None
            close_tile(*unit, *opened)
            opened = following
        for n in reversed(range(len(steps))):
            block = steps[n][0]
            acc = dot(values[...], weight[n])
            high, low = split(carry[n])
            tail = lax.broadcasted_iota(jnp.int32, (TAIL, pair), 0)
            tail = jnp.where(tail == 0, high.astype(f32), jnp.where(tail == 1, low.astype(f32), 0.0))
            for i in range(2):
                cols = slice(i * TILE, (i + 1) * TILE)
                out[2 * block + i, :HEAD_DIM] = acc[:, cols].astype(bf16)
                out[2 * block + i, HEAD_DIM:] = tail[:, cols].astype(bf16)

    last = out.shape[0] // 2 - 1
    block_steps(((row, True), (jnp.minimum(row + 1, last), False)))

    def later(step, _):
        block = row + 2 + 2 * step
        block_steps(((block, False), (jnp.minimum(block + 1, last), False)))
        return 0

    lax.fori_loop(0, lax.div(last - row, 2), later, 0)


def window_kernel(sinks, qw, prev, own, w_out, gain, keep, send):
    lane = lax.broadcasted_iota(jnp.int32, (TILE, TILE), 1)
    first = lane < HEAD_DIM
    block = lax.axis_index("z") + lax.axis_index("yy") + lax.axis_index("hy")
    query = qw[...].astype(f32)
    both = jnp.concatenate(
        [jnp.where(first, query, 0.0), jnp.where(first, pltpu.roll(query, HEAD_DIM, 1), 0.0)], axis=0
    ).astype(bf16)
    pair = jnp.concatenate([prev[...], own[...]], axis=0)
    logits = dot(both, pair, 1, 1) * SCALE
    r_i = lax.broadcasted_iota(jnp.int32, (2 * TILE, 2 * TILE), 0)
    c_i = lax.broadcasted_iota(jnp.int32, (2 * TILE, 2 * TILE), 1)
    distance = r_i % TILE + WINDOW - c_i
    usable = (distance >= 0) & (distance < WINDOW) & (c_i >= TILE * jnp.where(block > 0, 0, 1))
    logits = jnp.where(usable, logits, -jnp.inf)
    sink = jnp.where(r_i[:, :1] < TILE, sinks[0], sinks[1])
    top = jnp.maximum(jnp.max(logits, axis=1, keepdims=True), sink)
    powers = jnp.exp(logits - top)
    total = jnp.sum(powers, axis=1, keepdims=True) + jnp.exp(sink - top)
    weights = (powers / total).astype(bf16)
    mixed = dot(weights, pair)
    result = jnp.where(first, pltpu.roll(mixed[:TILE], HEAD_DIM, 1), mixed[TILE:]).astype(bf16).astype(f32)
    share(result, gain, w_out, keep, send)


def share(result, gain, w_out, keep, send):
    width = w_out.shape[1]
    ssq = jnp.sum(result * result, axis=1, keepdims=True)
    high, low = split(jnp.broadcast_to(ssq, (TILE, TILE)))
    lane = lax.broadcasted_iota(jnp.int32, (TILE, TILE), 1)
    squares = jnp.where(lane == 0, high.astype(f32), low.astype(f32))
    product = dot((result * gain[...]).astype(bf16), w_out[...])
    own = lax.axis_index("core") == 0
    rows = keep.shape[1]
    for value, cols in ((product, slice(0, width)), (squares, slice(width, width + TILE))):
        for at in range(keep.shape[0]):
            even = value[2 * at * rows : (2 * at + 1) * rows]
            odd = value[(2 * at + 1) * rows : (2 * at + 2) * rows]
            keep[at, :, cols] = jnp.where(own, even, odd).astype(bf16)
            send[at, :, cols] = jnp.where(own, odd, even).astype(bf16)


def combine_kernel(parts, gain, w_out, keep, send):
    count = parts.shape[0] // 2
    heads = []
    for h in range(2):
        later = jnp.zeros((1, TILE), f32)
        total = jnp.zeros((HEAD_DIM, TILE), f32)
        for z in reversed(range(count)):
            at = 2 * z + h
            total = total + parts[at, :HEAD_DIM].astype(f32) * jnp.exp2(-later)
            tail = parts[at, HEAD_DIM:].astype(f32)
            later = later + tail[0:1] + tail[1:2]
        heads.append(total)
    result = jnp.transpose(jnp.concatenate(heads, axis=0))
    share(result.astype(bf16).astype(f32), gain, w_out, keep, send)


def pairs_kernel(keep_s, came_s, keep_w, came_w, out):
    width = keep_s.shape[2] - TILE
    lane = lax.broadcasted_iota(jnp.int32, (keep_s.shape[1], TILE), 1)
    for at in range(out.shape[0]):
        parts = []
        for n, (keep, came) in enumerate(((keep_s, came_s), (keep_w, came_w))):
            both = keep[at].astype(f32) + came[at].astype(f32)
            out[at, :, n * width : (n + 1) * width] = both[:, :width].astype(bf16)
            parts += split(both[:, width : width + 1] + both[:, width + 1 : width + 2])
        tail = parts[-1].astype(f32)
        for n in reversed(range(len(parts) - 1)):
            tail = jnp.where(lane == n, parts[n].astype(f32), tail)
        out[at, :, 2 * width :] = tail.astype(bf16)


def final_kernel(parts, gain, out):
    width = out.shape[1]
    count = parts.shape[0]
    squares = sum(parts[i, :, 2 * width :].astype(f32) for i in range(count))
    stick = lax.rsqrt((squares[:, 0:1] + squares[:, 1:2]) / SB_WIDTH + epsilon)
    window = lax.rsqrt((squares[:, 2:3] + squares[:, 3:4]) / SW_WIDTH + epsilon)
    sum_s = sum(parts[i, :, :width].astype(f32) for i in range(count))
    sum_w = sum(parts[i, :, width : 2 * width].astype(f32) for i in range(count))
    combined = (sum_s * stick + sum_w * window).astype(bf16).astype(f32)
    mean = jnp.mean(combined * combined, axis=1, keepdims=True)
    out[...] = (combined * lax.rsqrt(mean + epsilon) * gain[...]).astype(bf16)


def shards(
    tokens,
    pre_gain,
    w_query_stick,
    w_key_stick,
    w_value_stick,
    w_query_window,
    w_key_window,
    w_value_window,
    stick_bias,
    sinks,
    stick_gain,
    window_gain,
    w_out_stick,
    w_out_window,
    post_gain,
):
    tok_rows, feats = tokens.shape
    nz, ntp = lax.axis_size("z"), lax.axis_size(TP)
    width = ntp * feats

    def swap(value, axis):
        return lax.all_to_all(value, axis, 0, 0, tiled=True)

    chips = lax.axis_size("x")
    from_chips = lax.all_to_all(jnp.broadcast_to(tokens[None], (chips, tok_rows, feats)), "x", 0, 0, tiled=True)
    gathered = lax.all_gather(from_chips, "core")
    head_pair = w_key_stick.shape[1]

    wide = jax.ShapeDtypeStruct((tok_rows, width), bf16)
    block = jax.ShapeDtypeStruct((tok_rows, head_pair), bf16)
    q_all, gained, scale = call(
        queries_kernel,
        (
            jax.ShapeDtypeStruct((nz, 2, HEAD_DIM, tok_rows), bf16),
            wide,
            jax.ShapeDtypeStruct((tok_rows, TILE), f32),
        ),
        [VM, HB, HB],
        scratch=[
            pltpu.VMEM((1, width), f32),
            pltpu.VMEM(w_query_stick.shape, bf16),
            pltpu.SemaphoreType.DMA((2,)),
        ],
    )(gathered, pre_gain.reshape(1, width), w_query_stick)
    q_col = swap(q_all.reshape(2 * nz, HEAD_DIM, tok_rows), ("z", "hy"))
    kv_all, q_win, kv_win = call(
        rest_kernel,
        (jax.ShapeDtypeStruct((ROWS, tok_rows, head_pair), bf16), block, block),
        [VM] * 2 + [HB] * 5,
        scratch=[
            pltpu.VMEM((width, 2 * head_pair), bf16),
            pltpu.VMEM(w_query_window.shape, bf16),
            pltpu.VMEM((2 * HEAD_DIM, width), bf16),
            pltpu.SemaphoreType.DMA((5,)),
        ],
    )(gained, scale, w_key_stick, w_value_stick, w_query_window, w_key_window.T, w_value_window.T)
    count = nz * ROWS
    previous = lax.ppermute(kv_win, ("z", "yy", "hy"), [(i, i + 1) for i in range(count - 1)])
    kv_row = swap(kv_all, ("yy", "hy"))
    rows = tok_rows // ntp
    halves = (jax.ShapeDtypeStruct((ntp // 2, rows, width + TILE), bf16),) * 2
    keep_w, send_w = call(window_kernel, halves, [SM] + [VM] * 5)(
        sinks, q_win, previous, kv_win, w_out_window, window_gain.reshape(1, -1)
    )

    def to_other_core(value):
        return lax.ppermute(value, "core", [(0, 1), (1, 0)])

    came_w = to_other_core(send_w)
    partial = call(
        stick_kernel,
        jax.ShapeDtypeStruct((2 * nz, HEAD_DIM + TAIL, TILE), bf16),
        [SM, VM, VM],
        scratch=[
            pltpu.VMEM((2, ROWS * TILE, 2 * TILE), bf16),
            pltpu.VMEM((ROWS * TILE, 2 * HEAD_DIM), bf16),
            pltpu.VMEM((HEAD_DIM, ROWS * TILE), bf16),
        ],
    )(stick_bias, q_col, kv_row)
    returned = swap(partial, ("z", "hy"))
    keep_s, send_s = call(combine_kernel, halves, [VM] * 3)(returned, stick_gain.reshape(1, -1), w_out_stick)
    came_s = to_other_core(send_s)
    sending = call(
        pairs_kernel, jax.ShapeDtypeStruct((ntp // 2, rows, 2 * width + TILE), bf16), [VM] * 4
    )(keep_s, came_s, keep_w, came_w)
    arrived = swap(sending, "x")
    return call(
        final_kernel, jax.ShapeDtypeStruct((rows, width), bf16), [VM, VM], keep=False
    )(arrived, post_gain.reshape(1, width))


def solution(mesh):
    cube = Mesh(
        mesh.devices.reshape(-1, ROWS // 2, 2, mesh.devices.shape[-1] // 2, 2), ("z", "yy", "hy", "x", "core")
    )
    seq = ("z", "yy", "hy")
    in_specs = (
        P(seq, TP),
        P(),
        P(None, TP),
        P(None, TP),
        P(None, TP),
        P(None, TP),
        P(None, TP),
        P(None, TP),
        P(TP),
        P(TP),
        P(TP),
        P(TP),
        P(TP, None),
        P(TP, None),
        P(),
    )
    out_specs = P((*seq, *TP), None)
    return jax.shard_map(shards, mesh=cube, in_specs=in_specs, out_specs=out_specs, check_vma=False)
```

```python
import jax
import jax.numpy as jnp
from jax import lax
from jax.experimental import pallas as pl
from jax.experimental.pallas import tpu as pltpu
from jax.sharding import Mesh, PartitionSpec as P


HEAD_DIM = 64
WINDOW = 128
TILE = 128
SB_WIDTH = 1024
SW_WIDTH = 1024
ROWS = 8
TAIL = 8
LOG2E = 1.4426950408889634
SCALE = HEAD_DIM ** (-0.5)

epsilon = 1e-06
TP = ("x", "core")
f32 = jnp.float32
bf16 = jnp.bfloat16

VM = pl.BlockSpec(memory_space=pltpu.VMEM)
SM = pl.BlockSpec(memory_space=pltpu.SMEM)
HB = pl.BlockSpec(memory_space=pltpu.HBM)


def call(kernel, out_shape, in_specs, scratch=(), keep=True):
    many = isinstance(out_shape, (tuple, list))
    shapes = out_shape if many else [out_shape]
    if keep:
        shapes = [pltpu.VMEM(s.shape, s.dtype) for s in shapes]
    run = pl.pallas_call(
        kernel,
        out_shape=shapes if many else shapes[0],
        in_specs=in_specs,
        out_specs=[VM] * len(shapes) if many else VM,
        scratch_shapes=list(scratch),
        compiler_params=pltpu.CompilerParams(vmem_limit_bytes=16 * 2**20),
    )

    def begun(*args):
        spaces = {id(VM): pltpu.VMEM, id(HB): pltpu.HBM}
        return run(
            *[
                pltpu.with_memory_space_constraint(a, spaces[id(spec)]) if id(spec) in spaces else a
                for a, spec in zip(args, in_specs)
            ]
        )

    return begun


def dot(a, b, ca=1, cb=0):
    return lax.dot_general(a, b, (((ca,), (cb,)), ((), ())), preferred_element_type=f32)


def split(value):
    high = value.astype(bf16)
    return high, (value - high.astype(f32)).astype(bf16)


def fetched(sources, targets, sems):
    copies = [pltpu.make_async_copy(s, t, sems.at[i]) for i, (s, t) in enumerate(zip(sources, targets))]
    for copy in copies:
        copy.start()
    return lambda at: copies[at].wait()


def queries_kernel(tok, gain, wq, q_out, normed_out, gains, held, sems):
    wait = fetched((gain, wq), (gains, held), sems)
    cores, chips, _, step = tok.shape
    wide = [tok[c, x].astype(f32) for x in range(chips) for c in range(cores)]
    total = sum(w * w for w in wide)
    scale = lax.rsqrt(jnp.sum(total, axis=1, keepdims=True) / (len(wide) * step) + epsilon)
    wait(0)
    for i, w in enumerate(wide):
        cols = slice(i * step, (i + 1) * step)
        normed_out[:, cols] = (w * scale * gains[:, cols]).astype(bf16)
    wait(1)
    query = dot(normed_out[...], held[...]).astype(bf16)
    turned = jnp.transpose(query.astype(f32)).astype(bf16)
    for i in range(q_out.shape[0]):
        q_out[i, 0] = turned[:HEAD_DIM]
        q_out[i, 1] = turned[HEAD_DIM:]


def rest_kernel(normed_in, wk, wv, wqw, wkw, wvw, kv_out, qw_out, kvw_out, both, held, narrow, sems):
    half = wk.shape[1]
    wait = fetched(
        (wk, wv, wqw, wkw, wvw),
        (both.at[:, :half], both.at[:, half:], held, narrow.at[:HEAD_DIM], narrow.at[HEAD_DIM:]),
        sems,
    )
    normed = normed_in[...]
    wait(3)
    wait(4)
    kvw_out[...] = dot(normed, narrow[...], 1, 1).astype(bf16)
    wait(0)
    wait(1)
    made = dot(normed, both[...])
    key, value = made[:, :half], made[:, half:]
    first = lax.broadcasted_iota(jnp.int32, (TILE, TILE), 1) < HEAD_DIM
    heads = [
        jnp.where(first, key, pltpu.roll(value, HEAD_DIM, 1)).astype(bf16),
        jnp.where(first, pltpu.roll(key, HEAD_DIM, 1), value).astype(bf16),
    ]
    for i in range(kv_out.shape[0]):
        kv_out[i] = heads[i % 2]
    wait(2)
    qw_out[...] = dot(normed, held[...]).astype(bf16)


def stick_kernel(bias, q, kv, out, weight, keys, values):
    row = lax.axis_index("z")
    duo = lax.axis_index("yy")
    shift = jnp.where(lax.axis_index("hy") == 0, bias[0], bias[1]) * LOG2E
    blocks = kv.shape[0]
    pair = 2 * TILE
    r_i = lax.broadcasted_iota(jnp.int32, (pair, pair), 0)
    c_i = lax.broadcasted_iota(jnp.int32, (pair, pair), 1)
    after = jnp.where(c_i > r_i, 1.0, 0.0).astype(bf16)
    for j in range(blocks):
        cols = slice(j * TILE, (j + 1) * TILE)
        both = kv[j].astype(f32)
        high, low = split(both[:, :HEAD_DIM] * (SCALE * LOG2E))
        keys[cols, :HEAD_DIM] = high
        keys[cols, HEAD_DIM:] = low
        values[:, cols] = jnp.transpose(both)[HEAD_DIM:].astype(bf16)

    def clear(block, _):
        out[2 * block] = jnp.zeros(out.shape[1:], bf16)
        out[2 * block + 1] = jnp.zeros(out.shape[1:], bf16)
        return 0

    lax.fori_loop(0, row, clear, 0)

    def block_steps(steps):
        queries = [jnp.concatenate([q[2 * b], q[2 * b + 1]], axis=1) for b, _ in steps]
        queries = [jnp.concatenate([v, v], axis=0) for v in queries]
        carry = [jnp.zeros((1, pair), f32) for _ in steps]

        def open_tile(n, j):
            s = dot(keys[j * TILE : (j + 2) * TILE], queries[n]) + shift
            soft = jnp.maximum(s, lax.log2(1.0 + jnp.exp2(jnp.minimum(s, 126.0))))
            rest = s - soft
            if steps[n][1]:
                seen = (j * TILE + r_i) < (duo * pair + c_i)
                soft = jnp.where(seen, soft, 0.0)
                rest = jnp.where(seen, rest, -jnp.inf)
            return rest, soft[:1], dot(after, soft.astype(bf16))

        def close_tile(n, j, rest, own, sums):
            w = jnp.exp2(rest - (sums + carry[n]))
            weight[n, j * TILE : (j + 2) * TILE] = w.astype(bf16)
            carry[n] = carry[n] + (sums[:1] + own)

        units = [(n, j) for j in reversed(range(0, blocks, 2)) for n in range(len(steps))]
        opened = open_tile(*units[0])
        for at, unit in enumerate(units):
            following = open_tile(*units[at + 1]) if at + 1 < len(units) else None
            close_tile(*unit, *opened)
            opened = following
        for n in reversed(range(len(steps))):
            block = steps[n][0]
            acc = dot(values[...], weight[n])
            high, low = split(carry[n])
            tail = lax.broadcasted_iota(jnp.int32, (TAIL, pair), 0)
            tail = jnp.where(tail == 0, high.astype(f32), jnp.where(tail == 1, low.astype(f32), 0.0))
            for i in range(2):
                cols = slice(i * TILE, (i + 1) * TILE)
                out[2 * block + i, :HEAD_DIM] = acc[:, cols].astype(bf16)
                out[2 * block + i, HEAD_DIM:] = tail[:, cols].astype(bf16)

    last = out.shape[0] // 2 - 1
    block_steps(((row, True), (jnp.minimum(row + 1, last), False)))

    def later(step, _):
        block = row + 2 + 2 * step
        block_steps(((block, False), (jnp.minimum(block + 1, last), False)))
        return 0

    lax.fori_loop(0, lax.div(last - row, 2), later, 0)


def window_kernel(sinks, qw, prev, own, w_out, gain, stick_gain, keep, send, stick_gain_out):
    stick_gain_out[...] = stick_gain[...]
    lane = lax.broadcasted_iota(jnp.int32, (TILE, TILE), 1)
    first = lane < HEAD_DIM
    block = lax.axis_index("z") + lax.axis_index("yy") + lax.axis_index("hy")
    query = qw[...].astype(f32)
    both = jnp.concatenate(
        [jnp.where(first, query, 0.0), jnp.where(first, pltpu.roll(query, HEAD_DIM, 1), 0.0)], axis=0
    ).astype(bf16)
    pair = jnp.concatenate([prev[...], own[...]], axis=0)
    logits = dot(both, pair, 1, 1) * SCALE
    r_i = lax.broadcasted_iota(jnp.int32, (2 * TILE, 2 * TILE), 0)
    c_i = lax.broadcasted_iota(jnp.int32, (2 * TILE, 2 * TILE), 1)
    distance = r_i % TILE + WINDOW - c_i
    usable = (distance >= 0) & (distance < WINDOW) & (c_i >= TILE * jnp.where(block > 0, 0, 1))
    logits = jnp.where(usable, logits, -jnp.inf)
    sink = jnp.where(r_i[:, :1] < TILE, sinks[0], sinks[1])
    top = jnp.maximum(jnp.max(logits, axis=1, keepdims=True), sink)
    powers = jnp.exp(logits - top)
    total = jnp.sum(powers, axis=1, keepdims=True) + jnp.exp(sink - top)
    weights = (powers / total).astype(bf16)
    mixed = dot(weights, pair)
    result = jnp.where(first, pltpu.roll(mixed[:TILE], HEAD_DIM, 1), mixed[TILE:]).astype(bf16).astype(f32)
    share(result, gain, w_out, keep, send)


def share(result, gain, w_out, keep, send):
    width = w_out.shape[1]
    ssq = jnp.sum(result * result, axis=1, keepdims=True)
    high, low = split(jnp.broadcast_to(ssq, (TILE, TILE)))
    lane = lax.broadcasted_iota(jnp.int32, (TILE, TILE), 1)
    squares = jnp.where(lane == 0, high.astype(f32), low.astype(f32))
    product = dot((result * gain[...]).astype(bf16), w_out[...])
    own = lax.axis_index("core") == 0
    rows = keep.shape[1]
    for value, cols in ((product, slice(0, width)), (squares, slice(width, width + TILE))):
        for at in range(keep.shape[0]):
            even = value[2 * at * rows : (2 * at + 1) * rows]
            odd = value[(2 * at + 1) * rows : (2 * at + 2) * rows]
            keep[at, :, cols] = jnp.where(own, even, odd).astype(bf16)
            send[at, :, cols] = jnp.where(own, odd, even).astype(bf16)


def combine_kernel(parts, gain, w_out, keep, send):
    count = parts.shape[0] // 2
    heads = []
    for h in range(2):
        later = jnp.zeros((1, TILE), f32)
        total = jnp.zeros((HEAD_DIM, TILE), f32)
        for z in reversed(range(count)):
            at = 2 * z + h
            total = total + parts[at, :HEAD_DIM].astype(f32) * jnp.exp2(-later)
            tail = parts[at, HEAD_DIM:].astype(f32)
            later = later + tail[0:1] + tail[1:2]
        heads.append(total)
    result = jnp.transpose(jnp.concatenate(heads, axis=0))
    share(result.astype(bf16).astype(f32), gain, w_out, keep, send)


def pairs_kernel(keep_s, came_s, keep_w, came_w, out):
    width = keep_s.shape[2] - TILE
    lane = lax.broadcasted_iota(jnp.int32, (keep_s.shape[1], TILE), 1)
    for at in range(out.shape[0]):
        parts = []
        for n, (keep, came) in enumerate(((keep_s, came_s), (keep_w, came_w))):
            both = keep[at].astype(f32) + came[at].astype(f32)
            out[at, :, n * width : (n + 1) * width] = both[:, :width].astype(bf16)
            parts += split(both[:, width : width + 1] + both[:, width + 1 : width + 2])
        tail = parts[-1].astype(f32)
        for n in reversed(range(len(parts) - 1)):
            tail = jnp.where(lane == n, parts[n].astype(f32), tail)
        out[at, :, 2 * width :] = tail.astype(bf16)


def final_kernel(parts, gain, out):
    width = out.shape[1]
    count = parts.shape[0]
    squares = sum(parts[i, :, 2 * width :].astype(f32) for i in range(count))
    stick = lax.rsqrt((squares[:, 0:1] + squares[:, 1:2]) / SB_WIDTH + epsilon)
    window = lax.rsqrt((squares[:, 2:3] + squares[:, 3:4]) / SW_WIDTH + epsilon)
    sum_s = sum(parts[i, :, :width].astype(f32) for i in range(count))
    sum_w = sum(parts[i, :, width : 2 * width].astype(f32) for i in range(count))
    combined = (sum_s * stick + sum_w * window).astype(bf16).astype(f32)
    mean = jnp.mean(combined * combined, axis=1, keepdims=True)
    out[...] = (combined * lax.rsqrt(mean + epsilon) * gain[...]).astype(bf16)


def shards(
    tokens,
    pre_gain,
    w_query_stick,
    w_key_stick,
    w_value_stick,
    w_query_window,
    w_key_window,
    w_value_window,
    stick_bias,
    sinks,
    stick_gain,
    window_gain,
    w_out_stick,
    w_out_window,
    post_gain,
):
    tok_rows, feats = tokens.shape
    nz, ntp = lax.axis_size("z"), lax.axis_size(TP)
    width = ntp * feats

    def swap(value, axis):
        return lax.all_to_all(value, axis, 0, 0, tiled=True)

    chips = lax.axis_size("x")
    from_chips = lax.all_to_all(jnp.broadcast_to(tokens[None], (chips, tok_rows, feats)), "x", 0, 0, tiled=True)
    gathered = lax.all_gather(from_chips, "core")
    head_pair = w_key_stick.shape[1]

    wide = jax.ShapeDtypeStruct((tok_rows, width), bf16)
    block = jax.ShapeDtypeStruct((tok_rows, head_pair), bf16)
    q_all, normed = call(
        queries_kernel,
        (jax.ShapeDtypeStruct((nz, 2, HEAD_DIM, tok_rows), bf16), wide),
        [VM, HB, HB],
        scratch=[
            pltpu.VMEM((1, width), f32),
            pltpu.VMEM(w_query_stick.shape, bf16),
            pltpu.SemaphoreType.DMA((2,)),
        ],
    )(gathered, pre_gain.reshape(1, width), w_query_stick)
    q_col = swap(q_all.reshape(2 * nz, HEAD_DIM, tok_rows), ("z", "hy"))
    kv_all, q_win, kv_win = call(
        rest_kernel,
        (jax.ShapeDtypeStruct((ROWS, tok_rows, head_pair), bf16), block, block),
        [VM] + [HB] * 5,
        scratch=[
            pltpu.VMEM((width, 2 * head_pair), bf16),
            pltpu.VMEM(w_query_window.shape, bf16),
            pltpu.VMEM((2 * HEAD_DIM, width), bf16),
            pltpu.SemaphoreType.DMA((5,)),
        ],
    )(normed, w_key_stick, w_value_stick, w_query_window, w_key_window.T, w_value_window.T)
    count = nz * ROWS
    previous = lax.ppermute(kv_win, ("z", "yy", "hy"), [(i, i + 1) for i in range(count - 1)])
    kv_row = swap(kv_all, ("yy", "hy"))
    rows = tok_rows // ntp
    halves = (jax.ShapeDtypeStruct((ntp // 2, rows, width + TILE), bf16),) * 2
    gain_row = jax.ShapeDtypeStruct((1, head_pair), f32)
    keep_w, send_w, stick_gain = call(window_kernel, (*halves, gain_row), [SM] + [VM] * 6)(
        sinks, q_win, previous, kv_win, w_out_window, window_gain.reshape(1, -1), stick_gain.reshape(1, -1)
    )

    def to_other_core(value):
        return lax.ppermute(value, "core", [(0, 1), (1, 0)])

    came_w = to_other_core(send_w)
    partial = call(
        stick_kernel,
        jax.ShapeDtypeStruct((2 * nz, HEAD_DIM + TAIL, TILE), bf16),
        [SM, VM, VM],
        scratch=[
            pltpu.VMEM((2, ROWS * TILE, 2 * TILE), bf16),
            pltpu.VMEM((ROWS * TILE, 2 * HEAD_DIM), bf16),
            pltpu.VMEM((HEAD_DIM, ROWS * TILE), bf16),
        ],
    )(stick_bias, q_col, kv_row)
    returned = swap(partial, ("z", "hy"))
    keep_s, send_s = call(combine_kernel, halves, [VM] * 3)(
        returned, stick_gain, w_out_stick
    )
    came_s = to_other_core(send_s)
    sending = call(
        pairs_kernel, jax.ShapeDtypeStruct((ntp // 2, rows, 2 * width + TILE), bf16), [VM] * 4
    )(keep_s, came_s, keep_w, came_w)
    arrived = swap(sending, "x")
    return call(
        final_kernel, jax.ShapeDtypeStruct((rows, width), bf16), [VM, VM], keep=False
    )(arrived, post_gain.reshape(1, width))


def solution(mesh):
    cube = Mesh(
        mesh.devices.reshape(-1, ROWS // 2, 2, mesh.devices.shape[-1] // 2, 2), ("z", "yy", "hy", "x", "core")
    )
    seq = ("z", "yy", "hy")
    in_specs = (
        P(seq, TP),
        P(),
        P(None, TP),
        P(None, TP),
        P(None, TP),
        P(None, TP),
        P(None, TP),
        P(None, TP),
        P(TP),
        P(TP),
        P(TP),
        P(TP),
        P(TP, None),
        P(TP, None),
        P(),
    )
    out_specs = P((*seq, *TP), None)
    return jax.shard_map(shards, mesh=cube, in_specs=in_specs, out_specs=out_specs, check_vma=False)
```

```python
import jax
import jax.numpy as jnp
from jax import lax
from jax.experimental import pallas as pl
from jax.experimental.pallas import tpu as pltpu
from jax.sharding import Mesh, PartitionSpec as P


HEAD_DIM = 64
WINDOW = 128
TILE = 128
SB_WIDTH = 1024
SW_WIDTH = 1024
ROWS = 8
TAIL = 8
LOG2E = 1.4426950408889634
SCALE = HEAD_DIM ** (-0.5)

epsilon = 1e-06
TP = ("x", "core")
f32 = jnp.float32
bf16 = jnp.bfloat16

VM = pl.BlockSpec(memory_space=pltpu.VMEM)
SM = pl.BlockSpec(memory_space=pltpu.SMEM)
HB = pl.BlockSpec(memory_space=pltpu.HBM)


def call(kernel, out_shape, in_specs, scratch=(), keep=True):
    many = isinstance(out_shape, (tuple, list))
    shapes = out_shape if many else [out_shape]
    if keep:
        shapes = [pltpu.VMEM(s.shape, s.dtype) for s in shapes]
    run = pl.pallas_call(
        kernel,
        out_shape=shapes if many else shapes[0],
        in_specs=in_specs,
        out_specs=[VM] * len(shapes) if many else VM,
        scratch_shapes=list(scratch),
        compiler_params=pltpu.CompilerParams(vmem_limit_bytes=16 * 2**20),
    )

    def begun(*args):
        spaces = {id(VM): pltpu.VMEM, id(HB): pltpu.HBM}
        return run(
            *[
                pltpu.with_memory_space_constraint(a, spaces[id(spec)]) if id(spec) in spaces else a
                for a, spec in zip(args, in_specs)
            ]
        )

    return begun


def dot(a, b, ca=1, cb=0):
    return lax.dot_general(a, b, (((ca,), (cb,)), ((), ())), preferred_element_type=f32)


def split(value):
    high = value.astype(bf16)
    return high, (value - high.astype(f32)).astype(bf16)


def fetched(sources, targets, sems):
    copies = [pltpu.make_async_copy(s, t, sems.at[i]) for i, (s, t) in enumerate(zip(sources, targets))]
    for copy in copies:
        copy.start()
    return lambda at: copies[at].wait()


def spread_kernel(tok, gain, wq, tok_out, gain_out, wq_out, sems):
    copies = [tok_out.at[i] for i in range(tok_out.shape[0])]
    wait = fetched((tok,) * len(copies) + (gain, wq), (*copies, gain_out, wq_out), sems)
    for i in range(len(copies) + 2):
        wait(i)


def queries_kernel(tok, gains, held, q_out, normed_out):
    cores, chips, _, step = tok.shape
    wide = [tok[c, x].astype(f32) for x in range(chips) for c in range(cores)]
    total = sum(w * w for w in wide)
    scale = lax.rsqrt(jnp.sum(total, axis=1, keepdims=True) / (len(wide) * step) + epsilon)
    for i, w in enumerate(wide):
        cols = slice(i * step, (i + 1) * step)
        normed_out[:, cols] = (w * scale * gains[:, cols]).astype(bf16)
    query = dot(normed_out[...], held[...]).astype(bf16)
    turned = jnp.transpose(query.astype(f32)).astype(bf16)
    for i in range(q_out.shape[0]):
        q_out[i, 0] = turned[:HEAD_DIM]
        q_out[i, 1] = turned[HEAD_DIM:]


def rest_kernel(normed_in, wk, wv, wqw, wkw, wvw, kv_out, qw_out, kvw_out, both, held, narrow, sems):
    half = wk.shape[1]
    wait = fetched(
        (wk, wv, wqw, wkw, wvw),
        (both.at[:, :half], both.at[:, half:], held, narrow.at[:HEAD_DIM], narrow.at[HEAD_DIM:]),
        sems,
    )
    normed = normed_in[...]
    wait(3)
    wait(4)
    kvw_out[...] = dot(normed, narrow[...], 1, 1).astype(bf16)
    wait(0)
    wait(1)
    made = dot(normed, both[...])
    key, value = made[:, :half], made[:, half:]
    first = lax.broadcasted_iota(jnp.int32, (TILE, TILE), 1) < HEAD_DIM
    heads = [
        jnp.where(first, key, pltpu.roll(value, HEAD_DIM, 1)).astype(bf16),
        jnp.where(first, pltpu.roll(key, HEAD_DIM, 1), value).astype(bf16),
    ]
    for i in range(kv_out.shape[0]):
        kv_out[i] = heads[i % 2]
    wait(2)
    qw_out[...] = dot(normed, held[...]).astype(bf16)


def stick_kernel(bias, q, kv, out, weight, keys, values):
    row = lax.axis_index("z")
    duo = lax.axis_index("yy")
    shift = jnp.where(lax.axis_index("hy") == 0, bias[0], bias[1]) * LOG2E
    blocks = kv.shape[0]
    pair = 2 * TILE
    r_i = lax.broadcasted_iota(jnp.int32, (pair, pair), 0)
    c_i = lax.broadcasted_iota(jnp.int32, (pair, pair), 1)
    after = jnp.where(c_i > r_i, 1.0, 0.0).astype(bf16)
    for j in range(blocks):
        cols = slice(j * TILE, (j + 1) * TILE)
        both = kv[j].astype(f32)
        high, low = split(both[:, :HEAD_DIM] * (SCALE * LOG2E))
        keys[cols, :HEAD_DIM] = high
        keys[cols, HEAD_DIM:] = low
        values[:, cols] = jnp.transpose(both)[HEAD_DIM:].astype(bf16)

    def clear(block, _):
        out[2 * block] = jnp.zeros(out.shape[1:], bf16)
        out[2 * block + 1] = jnp.zeros(out.shape[1:], bf16)
        return 0

    lax.fori_loop(0, row, clear, 0)

    def block_steps(steps):
        queries = [jnp.concatenate([q[2 * b], q[2 * b + 1]], axis=1) for b, _ in steps]
        queries = [jnp.concatenate([v, v], axis=0) for v in queries]
        carry = [jnp.zeros((1, pair), f32) for _ in steps]

        def open_tile(n, j):
            s = dot(keys[j * TILE : (j + 2) * TILE], queries[n]) + shift
            soft = jnp.maximum(s, lax.log2(1.0 + jnp.exp2(jnp.minimum(s, 126.0))))
            rest = s - soft
            if steps[n][1]:
                seen = (j * TILE + r_i) < (duo * pair + c_i)
                soft = jnp.where(seen, soft, 0.0)
                rest = jnp.where(seen, rest, -jnp.inf)
            return rest, soft[:1], dot(after, soft.astype(bf16))

        def close_tile(n, j, rest, own, sums):
            w = jnp.exp2(rest - (sums + carry[n]))
            weight[n, j * TILE : (j + 2) * TILE] = w.astype(bf16)
            carry[n] = carry[n] + (sums[:1] + own)

        units = [(n, j) for j in reversed(range(0, blocks, 2)) for n in range(len(steps))]
        opened = open_tile(*units[0])
        for at, unit in enumerate(units):
            following = open_tile(*units[at + 1]) if at + 1 < len(units) else None
            close_tile(*unit, *opened)
            opened = following
        for n in reversed(range(len(steps))):
            block = steps[n][0]
            acc = dot(values[...], weight[n])
            high, low = split(carry[n])
            tail = lax.broadcasted_iota(jnp.int32, (TAIL, pair), 0)
            tail = jnp.where(tail == 0, high.astype(f32), jnp.where(tail == 1, low.astype(f32), 0.0))
            for i in range(2):
                cols = slice(i * TILE, (i + 1) * TILE)
                out[2 * block + i, :HEAD_DIM] = acc[:, cols].astype(bf16)
                out[2 * block + i, HEAD_DIM:] = tail[:, cols].astype(bf16)

    last = out.shape[0] // 2 - 1
    block_steps(((row, True), (jnp.minimum(row + 1, last), False)))

    def later(step, _):
        block = row + 2 + 2 * step
        block_steps(((block, False), (jnp.minimum(block + 1, last), False)))
        return 0

    lax.fori_loop(0, lax.div(last - row, 2), later, 0)


def window_kernel(sinks, qw, prev, own, w_out, gain, stick_gain, keep, send, stick_gain_out):
    stick_gain_out[...] = stick_gain[...]
    lane = lax.broadcasted_iota(jnp.int32, (TILE, TILE), 1)
    first = lane < HEAD_DIM
    block = lax.axis_index("z") + lax.axis_index("yy") + lax.axis_index("hy")
    query = qw[...].astype(f32)
    both = jnp.concatenate(
        [jnp.where(first, query, 0.0), jnp.where(first, pltpu.roll(query, HEAD_DIM, 1), 0.0)], axis=0
    ).astype(bf16)
    pair = jnp.concatenate([prev[...], own[...]], axis=0)
    logits = dot(both, pair, 1, 1) * SCALE
    r_i = lax.broadcasted_iota(jnp.int32, (2 * TILE, 2 * TILE), 0)
    c_i = lax.broadcasted_iota(jnp.int32, (2 * TILE, 2 * TILE), 1)
    distance = r_i % TILE + WINDOW - c_i
    usable = (distance >= 0) & (distance < WINDOW) & (c_i >= TILE * jnp.where(block > 0, 0, 1))
    logits = jnp.where(usable, logits, -jnp.inf)
    sink = jnp.where(r_i[:, :1] < TILE, sinks[0], sinks[1])
    top = jnp.maximum(jnp.max(logits, axis=1, keepdims=True), sink)
    powers = jnp.exp(logits - top)
    total = jnp.sum(powers, axis=1, keepdims=True) + jnp.exp(sink - top)
    weights = (powers / total).astype(bf16)
    mixed = dot(weights, pair)
    result = jnp.where(first, pltpu.roll(mixed[:TILE], HEAD_DIM, 1), mixed[TILE:]).astype(bf16).astype(f32)
    share(result, gain, w_out, keep, send)


def share(result, gain, w_out, keep, send):
    width = w_out.shape[1]
    ssq = jnp.sum(result * result, axis=1, keepdims=True)
    high, low = split(jnp.broadcast_to(ssq, (TILE, TILE)))
    lane = lax.broadcasted_iota(jnp.int32, (TILE, TILE), 1)
    squares = jnp.where(lane == 0, high.astype(f32), low.astype(f32))
    product = dot((result * gain[...]).astype(bf16), w_out[...])
    own = lax.axis_index("core") == 0
    rows = keep.shape[1]
    for value, cols in ((product, slice(0, width)), (squares, slice(width, width + TILE))):
        for at in range(keep.shape[0]):
            even = value[2 * at * rows : (2 * at + 1) * rows]
            odd = value[(2 * at + 1) * rows : (2 * at + 2) * rows]
            keep[at, :, cols] = jnp.where(own, even, odd).astype(bf16)
            send[at, :, cols] = jnp.where(own, odd, even).astype(bf16)


def combine_kernel(parts, gain, w_out, keep, send):
    count = parts.shape[0] // 2
    heads = []
    for h in range(2):
        later = jnp.zeros((1, TILE), f32)
        total = jnp.zeros((HEAD_DIM, TILE), f32)
        for z in reversed(range(count)):
            at = 2 * z + h
            total = total + parts[at, :HEAD_DIM].astype(f32) * jnp.exp2(-later)
            tail = parts[at, HEAD_DIM:].astype(f32)
            later = later + tail[0:1] + tail[1:2]
        heads.append(total)
    result = jnp.transpose(jnp.concatenate(heads, axis=0))
    share(result.astype(bf16).astype(f32), gain, w_out, keep, send)


def pairs_kernel(keep_s, came_s, keep_w, came_w, out):
    width = keep_s.shape[2] - TILE
    lane = lax.broadcasted_iota(jnp.int32, (keep_s.shape[1], TILE), 1)
    other = 1 - lax.axis_index("core")
    for at in range(out.shape[0]):
        parts = []
        for n, (keep, came) in enumerate(((keep_s[at], came_s[other, at]), (keep_w[at], came_w[at]))):
            both = keep.astype(f32) + came.astype(f32)
            out[at, :, n * width : (n + 1) * width] = both[:, :width].astype(bf16)
            parts += split(both[:, width : width + 1] + both[:, width + 1 : width + 2])
        tail = parts[-1].astype(f32)
        for n in reversed(range(len(parts) - 1)):
            tail = jnp.where(lane == n, parts[n].astype(f32), tail)
        out[at, :, 2 * width :] = tail.astype(bf16)


def final_kernel(parts, gain, out):
    width = out.shape[1]
    count = parts.shape[0]
    squares = sum(parts[i, :, 2 * width :].astype(f32) for i in range(count))
    stick = lax.rsqrt((squares[:, 0:1] + squares[:, 1:2]) / SB_WIDTH + epsilon)
    window = lax.rsqrt((squares[:, 2:3] + squares[:, 3:4]) / SW_WIDTH + epsilon)
    sum_s = sum(parts[i, :, :width].astype(f32) for i in range(count))
    sum_w = sum(parts[i, :, width : 2 * width].astype(f32) for i in range(count))
    combined = (sum_s * stick + sum_w * window).astype(bf16).astype(f32)
    mean = jnp.mean(combined * combined, axis=1, keepdims=True)
    out[...] = (combined * lax.rsqrt(mean + epsilon) * gain[...]).astype(bf16)


def shards(
    tokens,
    pre_gain,
    w_query_stick,
    w_key_stick,
    w_value_stick,
    w_query_window,
    w_key_window,
    w_value_window,
    stick_bias,
    sinks,
    stick_gain,
    window_gain,
    w_out_stick,
    w_out_window,
    post_gain,
):
    tok_rows, feats = tokens.shape
    nz, ntp = lax.axis_size("z"), lax.axis_size(TP)
    width = ntp * feats

    def swap(value, axis):
        return lax.all_to_all(value, axis, 0, 0, tiled=True)

    chips = lax.axis_size("x")
    copies, gain, w_query = call(
        spread_kernel,
        (
            jax.ShapeDtypeStruct((chips, tok_rows, feats), bf16),
            jax.ShapeDtypeStruct((1, width), f32),
            jax.ShapeDtypeStruct(w_query_stick.shape, bf16),
        ),
        [HB] * 3,
        scratch=[pltpu.SemaphoreType.DMA((chips + 2,))],
    )(tokens, pre_gain.reshape(1, width), w_query_stick)
    from_chips = lax.all_to_all(copies, "x", 0, 0, tiled=True)
    gathered = lax.all_gather(from_chips, "core")
    head_pair = w_key_stick.shape[1]

    wide = jax.ShapeDtypeStruct((tok_rows, width), bf16)
    block = jax.ShapeDtypeStruct((tok_rows, head_pair), bf16)
    q_all, normed = call(
        queries_kernel, (jax.ShapeDtypeStruct((nz, 2, HEAD_DIM, tok_rows), bf16), wide), [VM] * 3
    )(gathered, gain, w_query)
    q_col = swap(q_all.reshape(2 * nz, HEAD_DIM, tok_rows), ("z", "hy"))
    kv_all, q_win, kv_win = call(
        rest_kernel,
        (jax.ShapeDtypeStruct((ROWS, tok_rows, head_pair), bf16), block, block),
        [VM] + [HB] * 5,
        scratch=[
            pltpu.VMEM((width, 2 * head_pair), bf16),
            pltpu.VMEM(w_query_window.shape, bf16),
            pltpu.VMEM((2 * HEAD_DIM, width), bf16),
            pltpu.SemaphoreType.DMA((5,)),
        ],
    )(normed, w_key_stick, w_value_stick, w_query_window, w_key_window.T, w_value_window.T)
    count = nz * ROWS
    previous = lax.ppermute(kv_win, ("z", "yy", "hy"), [(i, i + 1) for i in range(count - 1)])
    kv_row = swap(kv_all, ("yy", "hy"))
    rows = tok_rows // ntp
    halves = (jax.ShapeDtypeStruct((ntp // 2, rows, width + TILE), bf16),) * 2
    gain_row = jax.ShapeDtypeStruct((1, head_pair), f32)
    keep_w, send_w, stick_gain = call(window_kernel, (*halves, gain_row), [SM] + [VM] * 6)(
        sinks, q_win, previous, kv_win, w_out_window, window_gain.reshape(1, -1), stick_gain.reshape(1, -1)
    )

    def to_other_core(value):
        return lax.ppermute(value, "core", [(0, 1), (1, 0)])

    came_w = to_other_core(send_w)
    partial = call(
        stick_kernel,
        jax.ShapeDtypeStruct((2 * nz, HEAD_DIM + TAIL, TILE), bf16),
        [SM, VM, VM],
        scratch=[
            pltpu.VMEM((2, ROWS * TILE, 2 * TILE), bf16),
            pltpu.VMEM((ROWS * TILE, 2 * HEAD_DIM), bf16),
            pltpu.VMEM((HEAD_DIM, ROWS * TILE), bf16),
        ],
    )(stick_bias, q_col, kv_row)
    returned = swap(partial, ("z", "hy"))
    keep_s, send_s = call(combine_kernel, halves, [VM] * 3)(
        returned, stick_gain, w_out_stick
    )
    came_s = lax.all_gather(send_s, "core")
    sending = call(
        pairs_kernel, jax.ShapeDtypeStruct((ntp // 2, rows, 2 * width + TILE), bf16), [VM] * 4
    )(keep_s, came_s, keep_w, came_w)
    arrived = swap(sending, "x")
    return call(
        final_kernel, jax.ShapeDtypeStruct((rows, width), bf16), [VM, VM], keep=False
    )(arrived, post_gain.reshape(1, width))


def solution(mesh):
    cube = Mesh(
        mesh.devices.reshape(-1, ROWS // 2, 2, mesh.devices.shape[-1] // 2, 2), ("z", "yy", "hy", "x", "core")
    )
    seq = ("z", "yy", "hy")
    in_specs = (
        P(seq, TP),
        P(),
        P(None, TP),
        P(None, TP),
        P(None, TP),
        P(None, TP),
        P(None, TP),
        P(None, TP),
        P(TP),
        P(TP),
        P(TP),
        P(TP),
        P(TP, None),
        P(TP, None),
        P(),
    )
    out_specs = P((*seq, *TP), None)
    return jax.shard_map(shards, mesh=cube, in_specs=in_specs, out_specs=out_specs, check_vma=False)
```
